32 devices in a mesh: sp: 8 (over z, y), tp: 4 (over x, core).
Axes of the slice: x: 2, y: 2, z: 4, core: 2. Of those that a mesh axis runs over, the one named last changes fastest.
Arguments:
- stream: bfloat16 [8192, 2048], P(('sp', 'tp')), may hold values from -6 to 6
- query_rows: bfloat16 [8192, 1024], P('sp', 'tp'), may hold values from -6 to 6
- key_rows: bfloat16 [8192, 1024], P('sp', 'tp'), may hold values from -6 to 6
- value_rows: bfloat16 [8192, 2048], P('sp', 'tp'), may hold values from -6 to 6
- gate_rows: bfloat16 [8192, 2048], P('sp', 'tp'), may hold values from -6 to 6
- log_decay: float32 [8192, 1024], P('sp', 'tp'), may hold values from -1 to 0
- head_gain: float32 [256], replicated, may hold values from 0.1 to 1.9
- out_weight: bfloat16 [2048, 2048], P('tp'), may hold values from -0.125 to 0.125
- mix_gain: float32 [2048], replicated, may hold values from 0.1 to 1.9
- up_weight: bfloat16 [2048, 8192], P('sp', 'tp'), may hold values from -0.125 to 0.125
- down_weight: bfloat16 [2048, 8192], P('sp', 'tp'), may hold values from -0.0625 to 0.0625
Outputs:
- mixed_out: bfloat16 [8192, 2048], P(('sp', 'tp'))
The draws below stay inside these ranges and needn't reach their ends.
All inputs are finite; a program needn't handle non-finite values.
Results may differ from the reference program's by a relative error of at most 0.02.
Values may be sent and summed in bfloat16 or wider, within the bound.
A program may use at most 128 MiB of HBM per device.

```python
import jax
import jax.numpy as jnp
from jax import lax

D = 2048
HEADS = 8
KEY_CHANNELS = 128
DV = 256
FF = 8192
BLOCK = 64
TOK_DEV = 1024
TOKENS = 8192
N_TP = 4


def draw_log_decay(key, part):
    keys = jax.random.split(jax.random.fold_in(key, 7), 7)
    devices = TOKENS // TOK_DEV
    width = HEADS * KEY_CHANNELS
    fast_share = 0.5
    noise = jax.random.uniform(keys[4], (TOKENS, width), jnp.float32, 0.5, 1.5)
    fast_head = jax.random.uniform(keys[0], (HEADS,), jnp.float32) < fast_share
    fast_channel = jnp.repeat(fast_head, KEY_CHANNELS)
    slow_rate = jnp.exp(jax.random.uniform(keys[1], (width,), jnp.float32, jnp.log(0.1), jnp.log(0.5))) / TOKENS
    fast_rate = jnp.exp(jax.random.uniform(keys[2], (width,), jnp.float32, jnp.log(0.02), jnp.log(0.033)))
    base = jnp.where(fast_channel, fast_rate, slow_rate)
    device_factor = jnp.exp(jax.random.uniform(keys[3], (devices, HEADS), jnp.float32, jnp.log(0.5), jnp.log(2.0)))
    device_rows = jnp.repeat(jnp.repeat(device_factor, TOK_DEV, axis=0), KEY_CHANNELS, axis=1)
    decay_rates = base[None, :] * device_rows * noise
    spots = jax.random.randint(keys[5], (2,), 0, TOKENS)
    decay_losses = jax.random.uniform(keys[6], (2, HEADS), jnp.float32, 0.2, 0.4)
    block_hits = (jnp.arange(TOKENS)[:, None] == spots[None, :]).astype(jnp.float32)
    block_surge = jnp.dot(block_hits, jnp.log(1.0 - decay_losses))
    return (jnp.repeat(block_surge, KEY_CHANNELS, axis=1) - decay_rates).astype(jnp.float32)


def shard_levels(own_key, shape, shards, smallest, largest):
    level = 1.0
    for dim, blocks in shards:
        steps = jax.random.uniform(jax.random.fold_in(jax.random.fold_in(own_key, 6), dim), (blocks,), jnp.float32, smallest / len(shards), largest / len(shards))
        level = level * jnp.repeat(jnp.exp(steps), shape[dim] // blocks).reshape((-1,) + (1,) * (len(shape) - 1 - dim))
    return level


def centred(rng, extent, scale, most, pieces=(), held_as=jnp.bfloat16):
    result = scale * jax.random.normal(rng, extent, jnp.float32)
    if pieces:
        result = result * shard_levels(rng, extent, pieces, -0.22, 0.18)
    return jnp.clip(result, -most, most).astype(held_as)


def setup_inputs(seed: int = 0) -> dict:
    key_of = jax.random.split(jax.random.key(seed), 12)
    stream = centred(key_of[0], (TOKENS, D), 1.0, 6.0, ((0, 32),))
    query_rows = centred(key_of[1], (TOKENS, HEADS * KEY_CHANNELS), 1.0, 6.0, ((0, 8), (1, 4)))
    key_rows = centred(key_of[2], (TOKENS, HEADS * KEY_CHANNELS), 1.0, 6.0, ((0, 8), (1, 4)))
    value_rows = centred(key_of[3], (TOKENS, HEADS * DV), 1.0, 6.0, ((0, 8), (1, 4)))
    gate_rows = centred(key_of[4], (TOKENS, HEADS * DV), 1.0, 6.0, ((0, 8), (1, 4)))
    log_decay = draw_log_decay(jax.random.fold_in(key_of[11], 71), 0)
    head_gain = jnp.clip(1.0 + 0.18 * jax.random.normal(key_of[6], (DV,), jnp.float32), 0.1, 1.9)
    out_weight = centred(key_of[7], (HEADS * DV, D), (HEADS * DV) ** -0.5, 0.125, ((0, 4),))
    mix_gain = jnp.clip(1.0 + 0.18 * jax.random.normal(key_of[8], (D,), jnp.float32), 0.1, 1.9)
    up_weight = centred(key_of[9], (D, FF), D ** -0.5, 0.125, ((0, 8), (1, 4)))
    down_weight = centred(key_of[10], (D, FF), FF ** -0.5, 0.0625, ((0, 8), (1, 4)))
    return {"stream": stream, "query_rows": query_rows, "key_rows": key_rows, "value_rows": value_rows, "gate_rows": gate_rows, "log_decay": log_decay, "head_gain": head_gain, "out_weight": out_weight, "mix_gain": mix_gain, "up_weight": up_weight, "down_weight": down_weight}


EPS = 1e-06

def attention(query_rows, key_rows, value_rows, log_decay):
    count = TOKENS // BLOCK
    queries = query_rows.astype(jnp.float32).reshape(count, BLOCK, HEADS, KEY_CHANNELS) * KEY_CHANNELS ** (-0.5)
    keys_all = key_rows.astype(jnp.float32).reshape(count, BLOCK, HEADS, KEY_CHANNELS)
    values_all = value_rows.astype(jnp.float32).reshape(count, BLOCK, HEADS, DV)
    decay_rates = log_decay.astype(jnp.float32).reshape(count, BLOCK, HEADS, KEY_CHANNELS)

    def step(matrix_state, inputs):
        query_block, kee, value_block, rate = inputs
        cum = jnp.cumsum(rate, axis=0)
        last = cum[-1:]
        decayed_state = kee * jnp.exp(last - cum)
        state_update = jnp.einsum('qzx,qzf->zxf', decayed_state, value_block, precision=lax.Precision.HIGHEST)
        matrix_state = jnp.exp(last[0])[..., None] * matrix_state + state_update
        head_output = jnp.einsum('wle,leg->wlg', query_block, matrix_state, precision=lax.Precision.HIGHEST)
        return (matrix_state, head_output)
    start = jnp.zeros((HEADS, KEY_CHANNELS, DV), jnp.float32)
    _, outs = lax.scan(step, start, (queries, keys_all, values_all, decay_rates))
    return outs.reshape(TOKENS, HEADS, DV)

def feed_block(rows_in, up_weight, down_weight):
    pre = jnp.dot(rows_in, up_weight, preferred_element_type=jnp.float32)
    hidden = jnp.square(jax.nn.relu(pre)).astype(jnp.bfloat16)
    group = FF // N_TP
    grouped = hidden.astype(jnp.float32).reshape(rows_in.shape[0], N_TP, group)
    downs = down_weight.astype(jnp.float32).reshape(D, N_TP, group)
    parts = jnp.einsum('rjf,djf->jrd', grouped, downs)
    parts = lax.optimization_barrier(parts.astype(jnp.bfloat16)).astype(jnp.float32)
    return lax.optimization_barrier(jnp.sum(parts, axis=0))

def reference(stream, query_rows, key_rows, value_rows, gate_rows, log_decay, head_gain, out_weight, mix_gain, up_weight, down_weight):
    readout = attention(query_rows, key_rows, value_rows, log_decay)
    scaled = readout * lax.rsqrt(lax.optimization_barrier(jnp.mean(readout * readout, axis=-1, keepdims=True)) + EPS)
    gates = gate_rows.astype(jnp.float32).reshape(TOKENS, HEADS, DV)
    gated = scaled * head_gain.astype(jnp.float32) * jax.nn.silu(gates)
    heads_out = gated.reshape(TOKENS, HEADS * DV).astype(jnp.bfloat16)
    attn = jnp.dot(heads_out, out_weight, preferred_element_type=jnp.float32)
    mid = (stream.astype(jnp.float32) + attn).astype(jnp.bfloat16)
    midf = mid.astype(jnp.float32)
    normed = (midf * lax.rsqrt(lax.optimization_barrier(jnp.mean(midf * midf, axis=-1, keepdims=True)) + EPS) * mix_gain.astype(jnp.float32)).astype(jnp.bfloat16)
    blocks = normed.reshape(TOKENS // TOK_DEV, TOK_DEV, D)
    feed = lax.map(lambda rows_in: feed_block(rows_in, up_weight, down_weight), blocks).reshape(TOKENS, D)
    return (midf + feed).astype(jnp.bfloat16)
```

```python
import functools

import jax
import jax.numpy as jnp
from jax import lax
from jax.experimental import pallas as pl
from jax.experimental.pallas import tpu as pltpu
from jax.sharding import PartitionSpec as P


KEY_CHANNELS = 128
DV = 256
BLOCK = 64
EPS = 1e-06


NT = (((1,), (1,)), ((), ()))
TN = (((0,), (0,)), ((), ()))


def local_states(q_ref, k_ref, v_ref, ld_ref, out_ref, qd_ref, state_ref):
    count = q_ref.shape[0] // BLOCK
    row = lax.broadcasted_iota(jnp.int32, (BLOCK, BLOCK), 0)
    col = lax.broadcasted_iota(jnp.int32, (BLOCK, BLOCK), 1)
    later = (col > row).astype(jnp.float32)
    scale = KEY_CHANNELS ** (-0.5)
    state = jnp.zeros((DV, KEY_CHANNELS), jnp.float32)
    total = jnp.zeros((1, KEY_CHANNELS), jnp.float32)
    for c in range(count):
        rows = pl.ds(c * BLOCK, BLOCK)
        rates = ld_ref[rows, :]
        rest = jnp.dot(later, rates, precision=lax.Precision.HIGHEST, preferred_element_type=jnp.float32)
        last = jnp.sum(rates, axis=0, keepdims=True)
        keys = (k_ref[rows, :].astype(jnp.float32) * jnp.exp(rest)).astype(jnp.bfloat16)
        update = lax.dot_general(v_ref[rows, :], keys, TN, preferred_element_type=jnp.float32)
        state = state * jnp.exp(last) + update
        total = total + last
        q = q_ref[rows, :]
        out_ref[rows, :] = lax.dot_general(
            q, state.astype(jnp.bfloat16), NT, preferred_element_type=jnp.float32
        ) * scale
        qd_ref[rows, :] = (q.astype(jnp.float32) * (jnp.exp(total) * scale)).astype(jnp.bfloat16)
    state_ref[0, :DV, :] = state.astype(jnp.bfloat16)
    state_ref[0, DV:, :] = jnp.broadcast_to(jnp.exp(total), (16, KEY_CHANNELS)).astype(jnp.bfloat16)


def finish_heads(own_ref, qd_ref, state_ref, gate_ref, gain_ref, out_ref):
    readout = own_ref[...] + lax.dot_general(
        qd_ref[...], state_ref[0, :DV, :], NT, preferred_element_type=jnp.float32
    )
    scaled = readout * lax.rsqrt(jnp.mean(readout * readout, axis=-1, keepdims=True) + EPS)
    gates = gate_ref[...].astype(jnp.float32)
    out_ref[...] = (scaled * gain_ref[...] * (gates / (1.0 + jnp.exp(-gates)))).astype(jnp.bfloat16)


def attention_local(q, k, v, ld):
    rows = q.shape[0]
    heads = q.shape[1] // KEY_CHANNELS
    kb = pl.BlockSpec((rows, KEY_CHANNELS), lambda h: (0, h))
    vb = pl.BlockSpec((rows, DV), lambda h: (0, h))
    return pl.pallas_call(
        local_states,
        grid=(heads,),
        in_specs=[kb, kb, vb, kb],
        out_specs=[vb, kb, pl.BlockSpec((1, DV + 16, KEY_CHANNELS), lambda h: (h, 0, 0))],
        out_shape=[
            jax.ShapeDtypeStruct((rows, heads * DV), jnp.float32),
            jax.ShapeDtypeStruct((rows, heads * KEY_CHANNELS), jnp.bfloat16),
            jax.ShapeDtypeStruct((heads, DV + 16, KEY_CHANNELS), jnp.bfloat16),
        ],
        cost_estimate=pl.CostEstimate(flops=6_000_000_000, bytes_accessed=8_000_000, transcendentals=0),
        name="local_states",
    )(q, k, v, ld)


def attention_finish(own, qd, state, gates, gain):
    rows = own.shape[0]
    heads = own.shape[1] // DV
    tile = rows // 2
    vb = pl.BlockSpec((tile, DV), lambda h, r: (r, h))
    return pl.pallas_call(
        finish_heads,
        grid=(heads, rows // tile),
        in_specs=[
            vb,
            pl.BlockSpec((tile, KEY_CHANNELS), lambda h, r: (r, h)),
            pl.BlockSpec((1, DV + 16, KEY_CHANNELS), lambda h, r: (h, 0, 0)),
            vb,
            pl.BlockSpec((1, DV), lambda h, r: (0, 0)),
        ],
        out_specs=vb,
        out_shape=jax.ShapeDtypeStruct(own.shape, jnp.bfloat16),
        cost_estimate=pl.CostEstimate(flops=3_000_000_000, bytes_accessed=4_000_000, transcendentals=0),
        name="finish_heads",
    )(own, qd, state, gates, gain)


def join(earlier, later):
    e, f = earlier.astype(jnp.float32), later.astype(jnp.float32)
    decay = f[:, DV : DV + 1]
    return jnp.concatenate(
        [decay * e[:, :DV] + f[:, :DV], jnp.broadcast_to(decay * e[:, DV : DV + 1], e[:, DV:].shape)], axis=1
    ).astype(jnp.bfloat16)


def shifted(a, by, n):
    return lax.ppermute(a, "sp", [(i, i + by) for i in range(n - by)])


def cycle_of(n):
    return list(range(0, n, 2)) + list(range(n - 1 - n % 2, 0, -2))


class Ring:
    def __init__(self, piece, n):
        self.n, self.cyc, self.piece = n, cycle_of(n), piece
        self.fwd = [(self.cyc[i], self.cyc[(i + 1) % n]) for i in range(n)]
        self.bwd = [(b, a) for a, b in self.fwd]
        self.left = self.right = piece
        self.hops = n // 2

    def hop(self, h):
        left, right = self.left, self.right
        if h == self.hops:
            half = self.piece.shape[0] // 2
            left, right = left[:half], right[half:]
        self.left = lax.ppermute(left, "sp", self.fwd)
        self.right = lax.ppermute(right, "sp", self.bwd)
        if h == self.hops:
            return [jnp.concatenate([self.left, self.right], axis=0)]
        return [self.left, self.right]


def owner_of(n, h):
    cyc = cycle_of(n)
    place = [0] * n
    for i, d in enumerate(cyc):
        place[d] = i
    me = jnp.asarray(place, jnp.int32)[lax.axis_index("sp")]
    cyc = jnp.asarray(cyc, jnp.int32)
    if h == 0:
        return [cyc[me]]
    back = cyc[(me - h) % n]
    return [back] if 2 * h == n else [back, cyc[(me + h) % n]]


def local(
    n_sp, n_tp, stream, query_rows, key_rows, value_rows, gate_rows, log_decay, head_gain, out_weight, mix_gain,
    up_weight, down_weight,
):
    nx = n_tp // 2
    own_rows = stream.shape[0]
    me = lax.axis_index("tp")
    x, core = me // 2, me % 2

    def across(a, dx):
        return lax.ppermute(a, "tp", [(((i // 2 + dx) % nx) * 2 + i % 2, i) for i in range(n_tp)])

    def swap(a):
        return lax.ppermute(a, "tp", [(i ^ 1, i) for i in range(n_tp)])

    up = Ring(up_weight, n_sp)
    down = Ring(down_weight, n_sp)
    width = up_weight.shape[0]
    up_full = lax.dynamic_update_slice_in_dim(
        jnp.zeros((width * n_sp, up_weight.shape[1]), up_weight.dtype), up_weight, owner_of(n_sp, 0)[0] * width, 0
    )
    ups = [up.hop(1)]
    downs = [[down_weight]]

    def tie(a, ring):
        a, ring.left, ring.right = lax.optimization_barrier((a, ring.left, ring.right))
        return a

    w = {(0, 0): out_weight}
    for dx in range(1, nx):
        w[dx, 0] = across(out_weight, dx)
    for dx in range(nx):
        w[dx, 1] = swap(w[dx, 0])

    own, qd, summary = attention_local(query_rows, key_rows, value_rows, log_decay)
    before, covered = tie(shifted(summary, 1, n_sp), up), 1
    while covered < n_sp - 1:
        wider = join(before, summary)
        if len(ups) < up.hops - 1:
            ups.append(up.hop(len(ups) + 1))
        before, covered = join(shifted(wider, covered + 1, n_sp), before), 2 * covered + 1
        before = tie(before, up)
    while len(ups) < up.hops:
        ups.append(up.hop(len(ups) + 1))
    before, down.left, down.right = lax.optimization_barrier((before, down.left, down.right))
    downs.append(down.hop(1))
    heads_out = attention_finish(own, qd, before, gate_rows, head_gain.reshape(1, DV))

    attn = None
    for dx in range(nx):
        for dc in range(2):
            to = ((x - dx) % nx) * 2 + (core + dc) % 2
            block = lax.dynamic_slice_in_dim(heads_out, to * own_rows, own_rows, 0)
            if (dx, dc) != (0, 0):
                block = lax.ppermute(
                    block, "tp", [(((i // 2 + dx) % nx) * 2 + (i % 2 + dc) % 2, i) for i in range(n_tp)]
                )
            term = jnp.dot(block, w[dx, dc], preferred_element_type=jnp.float32)
            attn = term if attn is None else attn + term
    midf = (stream.astype(jnp.float32) + attn).astype(jnp.bfloat16).astype(jnp.float32)
    normed = (
        midf * lax.rsqrt(jnp.mean(midf * midf, axis=-1, keepdims=True) + EPS) * mix_gain
    ).astype(jnp.bfloat16)

    normed = tie(normed, down)
    downs.append(down.hop(2))

    for h, pieces in enumerate(ups, 1):
        for piece, who in zip(pieces, owner_of(n_sp, h)):
            up_full = lax.dynamic_update_slice_in_dim(up_full, piece, who * width, 0)

    n = {(0, 0): normed}
    for dx in range(1, nx):
        n[dx, 0] = across(normed, dx)
    for dx in range(nx):
        n[dx, 1] = swap(n[dx, 0])
    n[nx - 1, 1] = tie(n[nx - 1, 1], down)
    while len(downs) <= down.hops:
        downs.append(down.hop(len(downs)))
    order = [(dx, dc) for dc in range(2) for dx in range(nx)]

    def hidden_of(rows):
        pre = jnp.dot(rows, up_full, preferred_element_type=jnp.float32)
        return jnp.square(jax.nn.relu(pre)).astype(jnp.bfloat16)

    hiddens = []
    for key in order:
        hiddens.append(hidden_of(n[key]))
    hidden = jnp.concatenate(hiddens, axis=0)

    out = jnp.zeros(stream.shape, jnp.bfloat16)
    mid = midf.astype(jnp.bfloat16)
    for h, pieces in enumerate(downs):
        whole = jnp.concatenate(pieces, axis=0) if len(pieces) > 1 else pieces[0]
        part = lax.dot_general(hidden, whole, NT, preferred_element_type=jnp.float32).astype(jnp.bfloat16)
        hidden, part = lax.optimization_barrier((hidden, part))
        half = nx * own_rows
        both = part[:half].astype(jnp.float32) + swap(part[half:]).astype(jnp.float32)
        feed = both[:own_rows]
        for dx in range(1, nx):
            send = both[dx * own_rows : (dx + 1) * own_rows].astype(jnp.bfloat16)
            feed = feed + across(send, nx - dx).astype(jnp.float32)
        for j, who in enumerate(owner_of(n_sp, h)):
            cols = lax.dynamic_slice_in_dim(mid, who * width, width, 1).astype(jnp.float32)
            done = (cols + feed[:, j * width : (j + 1) * width]).astype(jnp.bfloat16)
            out = lax.dynamic_update_slice_in_dim(out, done, who * width, 1)
    return out


TILE = 256
MESH = pl.DeviceIdType.MESH


class Links:
    def __init__(self, n_sp):
        self.sp, self.tp = lax.axis_index("sp"), lax.axis_index("tp")
        self.nz = n_sp // 2
        self.z, self.y = self.sp // 2, self.sp % 2
        self.x, self.c = self.tp // 2, self.tp % 2
        self.core = (self.sp, self.x * 2 + 1 - self.c)
        self.xn = (self.sp, (1 - self.x) * 2 + self.c)
        self.xo = (self.sp, (1 - self.x) * 2 + 1 - self.c)
        self.yn = (self.z * 2 + 1 - self.y, self.tp)

    def at_z(self, z):
        return (z * 2 + self.y, self.tp)

    def piece(self, s):
        z, n = self.z, self.nz
        near = jnp.minimum(z, n - 1 - z)
        turn = jnp.where(s % 2 == 1, z - (s + 1) // 2, z + s // 2)
        rest = jnp.where(z < n - 1 - z, s, n - 1 - s)
        return jnp.where(s <= 2 * near, turn, rest)


def remote(src, dst, send, recv, dev):
    return pltpu.make_async_remote_copy(
        src_ref=src, dst_ref=dst, send_sem=send, recv_sem=recv, device_id=dev, device_id_type=MESH
    )


def layer_kernel(
    n_sp, n_tp, stream, query, key, value, gate, rates_in, head_gain, mix_gain, out_w, up_w, down_w, out,
    up, down, wo, qv, kv, vv, gv, ldv, own, qd, state, total, summ, peer, tsend, trecv, prefix, bsend, before,
    heads, hrecv, acts, hidden, mid, psend, pown, sum_x, sum_y, pass_y, pass_x, outv,
    ld_s, zown_s, zfwd_s, z_r, y_s, y_r, d_s, d_r, wo_s, wo_r, s_s, s_r, t_s, t_r, h_s, h_r, a_s, a_r, p_s, p_r, o_s,
):
    f32, bf16 = jnp.float32, jnp.bfloat16
    L = Links(n_sp)
    z, y, c, nz = L.z, L.y, L.c, L.nz
    rows, width = stream.shape
    span = query.shape[0]
    n_heads = query.shape[1] // KEY_CHANNELS
    slab, half = up_w.shape[0], up_w.shape[1] // 2
    half_rows = rows // 2
    np_ = 2 * nz

    loads = [(query, qv), (key, kv), (value, vv), (rates_in, ldv)]
    first = [pltpu.make_async_copy(a, b, ld_s.at[i]) for i, (a, b) in enumerate(loads)]
    for cp in first:
        cp.start()
    barrier = pltpu.get_barrier_semaphore()
    partners = [L.core, L.xn, L.xo, L.yn] + [L.at_z((z + k) % nz) for k in range(1, nz)]
    for dev in partners:
        pl.semaphore_signal(barrier, inc=1, device_id=dev, device_id_type=MESH)
    pl.semaphore_wait(barrier, len(partners))

    bufs, source = (up, down), (up_w, down_w)

    def place(kind, core, j, part):
        row = j * 2 + (part if kind else (y + part) % 2)
        return bufs[kind].at[core, pl.ds(pl.multiple_of(row * slab, slab), slab), :]

    def halfcols(kind, h):
        return source[kind].at[:, pl.ds(pl.multiple_of(h * half, half), half)]

    def own_rows(kind, yy):
        return bufs[kind].at[c, pl.ds(pl.multiple_of((z * 2 + yy) * slab, slab), slab), :]

    keep = [pltpu.make_async_copy(halfcols(k, y), own_rows(k, y), ld_s.at[6 + k]) for k in range(2)]
    cross = [
        remote(halfcols(k, 1 - y), own_rows(k, y), y_s.at[k], y_r.at[k], L.yn) for k in range(2)
    ]

    def to_side(kind, part, side):
        to = z + (1 if side else -1)
        src = halfcols(0, y) if (kind, part) == (0, 0) else place(kind, c, z, part)
        return remote(src, place(kind, c, z, part), zown_s.at[kind, part, side], z_r.at[kind, z, part], L.at_z((to + nz) % nz))

    def to_core(kind, j, part, from_hbm=False):
        dst = place(kind, c, j, part)
        return remote(halfcols(kind, y) if from_hbm else dst, dst, d_s.at[kind, j, part], d_r.at[kind, j, part], L.core)

    def send_own(kind, part, sides=(0, 1)):
        for side in sides:
            @pl.when((z < nz - 1) if side else (z > 0))
            def _():
                to_side(kind, part, side).start()

    def open_part(part):
        if part == 0:
            keep[0].start()
        else:
            cross[0].wait_recv()
        to_core(0, z, part, part == 0).start()

    def onward(kind, j, part):
        to = jnp.where(j < z, z + 1, z - 1)
        dst = place(kind, c, j, part)
        return remote(dst, dst, zfwd_s.at[kind, j, part], z_r.at[kind, j, part], L.at_z((to + nz) % nz))

    inner = jnp.logical_and(z > 0, z < nz - 1)
    edge = jnp.logical_or(z == 0, z == nz - 1)

    def arrive(kind, s, part, forward):
        j = L.piece(s)
        cp = onward(kind, j, part)
        cp.wait_recv()
        if forward:
            cp.start()
        to_core(kind, j, part).start()

    def forward_inner(kind, s, part):
        @pl.when(inner)
        def _():
            arrive(kind, s, part, True)

    def from_core(kind, j, part):
        dst = place(kind, 1 - c, j, part)
        return remote(dst, dst, d_s.at[kind, j, part], d_r.at[kind, j, part], L.core)

    cross[0].start()
    send_own(0, 0)
    wo_own = pltpu.make_async_copy(out_w, wo.at[L.tp], ld_s.at[4])
    wo_x = remote(out_w, wo.at[L.tp], wo_s.at[0], wo_r.at[0], L.xn)
    wo_c = remote(out_w, wo.at[L.tp], wo_s.at[1], wo_r.at[1], L.core)
    wo_x.start()
    wo_c.start()
    wo_own.start()
    open_part(0)
    keep[1].start()
    late = [pltpu.make_async_copy(gate, gv, ld_s.at[5]), pltpu.make_async_copy(stream, mid, ld_s.at[8])]
    for cp in late:
        cp.start()

    row = lax.broadcasted_iota(jnp.int32, (BLOCK, BLOCK), 0)
    col = lax.broadcasted_iota(jnp.int32, (BLOCK, BLOCK), 1)
    later = (col > row).astype(f32)
    scale = KEY_CHANNELS ** (-0.5)
    state[...] = jnp.zeros_like(state)
    total[...] = jnp.zeros_like(total)
    for cp in first:
        cp.wait()

    def block(i, carry):
        at = pl.ds(pl.multiple_of(i * BLOCK, BLOCK), BLOCK)
        for h in range(n_heads):
            ks, vs = pl.ds(h * KEY_CHANNELS, KEY_CHANNELS), pl.ds(h * DV, DV)
            rates = ldv[at, ks]
            rest = jnp.dot(later, rates, precision=lax.Precision.HIGHEST, preferred_element_type=f32)
            last = jnp.sum(rates, axis=0, keepdims=True)
            keys = (kv[at, ks].astype(f32) * jnp.exp(rest)).astype(bf16)
            update = lax.dot_general(vv[at, vs], keys, TN, preferred_element_type=f32)
            new = state[h] * jnp.exp(last) + update
            state[h] = new
            tot = total[h] + last
            total[h] = tot
            q = qv[at, ks]
            own[at, vs] = lax.dot_general(q, new.astype(bf16), NT, preferred_element_type=f32) * scale
            qd[at, ks] = (q.astype(f32) * (jnp.exp(tot) * scale)).astype(bf16)
        return carry

    lax.fori_loop(0, span // BLOCK, block, 0, unroll=2)
    for h in range(n_heads):
        summ[h, :DV, :] = state[h].astype(bf16)
        summ[h, DV:, :] = jnp.broadcast_to(jnp.exp(total[h]), (16, KEY_CHANNELS)).astype(bf16)

    swap = remote(summ.at[1 - y], peer, s_s.at[0], s_r.at[0], L.yn)
    swap.start()
    open_part(1)
    send_own(0, 1)
    swap.wait_recv()
    mine, other = summ[y].astype(f32), peer[...].astype(f32)
    is0 = y == 0
    early, late_ = jnp.where(is0, mine, other), jnp.where(is0, other, mine)
    dec = late_[DV : DV + 1]
    tsend[:DV, :] = (dec * early[:DV] + late_[:DV]).astype(bf16)
    tsend[DV:, :] = (dec * early[DV:]).astype(bf16)

    def hand_on(zz):
        return remote(tsend, trecv.at[z], t_s.at[zz], t_r.at[z], L.at_z(zz))

    for zz in range(1, nz):
        @pl.when(z < zz)
        def _():
            hand_on(zz).start()
    forward_inner(0, 1, 0)
    forward_inner(0, 2, 0)
    prefix[...] = jnp.zeros_like(prefix)
    for j in range(nz - 1):
        @pl.when(j < z)
        def _():
            remote(tsend, trecv.at[j], t_s.at[j], t_r.at[j], L.at_z(j)).wait_recv()
            got = trecv[j].astype(f32)
            prefix[...] = got[DV : DV + 1] * prefix[...] + got[:DV]
    whole = prefix[...]
    first_y = jnp.where(is0, mine, other)
    onto = first_y[DV : DV + 1] * whole + first_y[:DV]
    bsend[...] = jnp.where(is0, onto, whole).astype(bf16)
    before[y] = jnp.where(is0, whole, onto).astype(bf16)
    back = remote(bsend, before.at[y], s_s.at[1], s_r.at[1], L.yn)
    back.start()
    forward_inner(0, 1, 1)
    forward_inner(0, 2, 1)
    remote(bsend, before.at[1 - y], s_s.at[1], s_r.at[1], L.yn).wait_recv()
    cross[1].start()

    late[0].wait()
    gain = head_gain[...]

    def finish(t):
        for r in range(0, rows, 128):
            at = pl.ds(pl.multiple_of(t * rows + r, 128), 128)
            for h in range(n_heads):
                ks, vs = pl.ds(h * KEY_CHANNELS, KEY_CHANNELS), pl.ds(h * DV, DV)
                readout = own[at, vs] + lax.dot_general(qd[at, ks], before[h], NT, preferred_element_type=f32)
                scaled = readout * lax.rsqrt(jnp.mean(readout * readout, axis=-1, keepdims=True) + EPS)
                g = gv[at, vs].astype(f32)
                heads[t, pl.ds(r, 128), vs] = (scaled * gain * (g / (1.0 + jnp.exp(-g)))).astype(bf16)

    head_sends = []
    for i, dev in enumerate((L.xn, L.xo, L.core)):
        t = dev[1]
        finish(t)
        cp = remote(heads.at[t], hrecv.at[L.tp], h_s.at[i], h_r.at[i], dev)
        cp.start()
        head_sends.append(cp)
    finish(L.tp)
    hrecv[L.tp] = heads[L.tp]
    forward_inner(0, 3, 0)

    wo_from_x = remote(out_w, wo.at[L.xn[1]], wo_s.at[0], wo_r.at[0], L.xn)
    wo_from_x.wait_recv()
    relay = remote(wo.at[L.xn[1]], wo.at[L.xn[1]], wo_s.at[2], wo_r.at[2], L.core)
    relay.start()
    keep[1].wait()
    cross[1].wait_recv()
    for part in range(2):
        send_own(1, part)
        to_core(1, z, part).start()
    remote(out_w, wo.at[L.core[1]], wo_s.at[1], wo_r.at[1], L.core).wait_recv()
    remote(wo.at[L.xo[1]], wo.at[L.xo[1]], wo_s.at[2], wo_r.at[2], L.core).wait_recv()
    wo_own.wait()
    late[1].wait()
    for i, dev in enumerate((L.xn, L.xo, L.core)):
        remote(heads.at[dev[1]], hrecv.at[dev[1]], h_s.at[i], h_r.at[i], dev).wait_recv()
    forward_inner(0, 3, 1)

    square = jnp.zeros((rows, 1), f32)
    wide = min(512, width)
    for n in range(0, width, wide):
        cols = pl.ds(n, wide)
        acc = mid[:, cols].astype(f32)
        for t in range(n_tp):
            acc = acc + jnp.dot(hrecv[t], wo[t, :, cols], preferred_element_type=f32)
        m = acc.astype(bf16)
        mid[:, cols] = m
        m = m.astype(f32)
        square = square + jnp.sum(m * m, axis=-1, keepdims=True)
    norm = lax.rsqrt(square * (1.0 / width) + EPS)
    for n in range(0, width, wide):
        cols = pl.ds(n, wide)
        acts[0, :, cols] = (mid[:, cols].astype(f32) * norm * mix_gain[:, cols]).astype(bf16)

    halves = (pl.ds(0, half_rows), pl.ds(half_rows, half_rows))

    def act_copy(i):
        slot, part, dst, dev = [(0, 0, 1, L.xn), (0, 1, 1, L.xn), (0, 0, 2, L.yn), (0, 1, 2, L.yn), (1, 0, 3, L.yn), (2, 1, 3, L.xn)][i]
        return remote(acts.at[slot, halves[part], :], acts.at[dst, halves[part], :], a_s.at[i], a_r.at[i], dev)

    for i in (0, 3, 1, 2):
        act_copy(i).start()

    for s in range(1, nz):
        for part in range(2):
            @pl.when(edge)
            def _():
                arrive(0, s, part, False)

    def up_rows(i):
        def step(n, carry):
            core = n // (half // TILE)
            at = pl.ds(pl.multiple_of((n % (half // TILE)) * TILE, TILE), TILE)
            pre = jnp.dot(acts[i], up[core, :, at], preferred_element_type=f32)
            pre = jnp.maximum(pre, 0.0)
            hidden[i, :, pl.ds(pl.multiple_of(n * TILE, TILE), TILE)] = (pre * pre).astype(bf16)
            return carry

        lax.fori_loop(0, 2 * half // TILE, step, 0)

    keep[0].wait()
    for j in range(nz):
        for part in range(2):
            from_core(0, j, part).wait_recv()
    up_rows(0)
    forward_inner(1, 1, 0)
    forward_inner(1, 2, 0)
    act_copy(0).wait_recv()
    act_copy(4).start()
    act_copy(3).wait_recv()
    act_copy(5).start()
    act_copy(1).wait_recv()
    up_rows(1)
    forward_inner(1, 1, 1)
    forward_inner(1, 2, 1)
    act_copy(2).wait_recv()
    up_rows(2)
    forward_inner(1, 3, 0)
    act_copy(4).wait_recv()
    act_copy(5).wait_recv()
    up_rows(3)
    forward_inner(1, 3, 1)

    a, b = halves

    def columns(t):
        d = L.piece(t // 2) * 2 + t % 2
        return d, pl.ds(pl.multiple_of(d * slab, slab), slab)

    def part_copy(i, t):
        d, cols = columns(t)
        src, dst, dev = [
            (psend.at[2, a, cols], pass_y.at[:, cols], L.yn),
            (psend.at[2, b, cols], pass_x.at[:, cols], L.xn),
            (psend.at[0, b, cols], sum_x.at[b, cols], L.xn),
            (psend.at[1, a, cols], sum_y.at[a, cols], L.yn),
            (psend.at[0, a, cols], sum_x.at[a, cols], L.xn),
            (psend.at[1, b, cols], sum_y.at[b, cols], L.yn),
        ][i]
        return remote(src, dst, p_s.at[i, d], p_r.at[i, d], dev)

    def down_step(t, carry):
        @pl.when(t < np_)
        def _():
            s, part = t // 2, t % 2
            j = L.piece(s)

            @pl.when(jnp.logical_and(edge, t >= 2))
            def _():
                arrive(1, s, part, False)

            from_core(1, j, part).wait_recv()
            _, cols = columns(t)
            w0, w1 = place(1, 0, j, part), place(1, 1, j, part)

            def rows_of(i):
                return lax.dot_general(
                    hidden[i, :, :half], w0[...], NT, preferred_element_type=f32
                ) + lax.dot_general(hidden[i, :, half:], w1[...], NT, preferred_element_type=f32)

            psend[2, :, cols] = rows_of(3).astype(bf16)
            part_copy(0, t).start()
            part_copy(1, t).start()
            psend[0, :, cols] = rows_of(1).astype(bf16)
            part_copy(2, t).start()
            psend[1, :, cols] = rows_of(2).astype(bf16)
            part_copy(3, t).start()
            pown[:, cols] = rows_of(0)

        @pl.when(jnp.logical_and(t >= 1, t < np_ + 1))
        def _():
            u = t - 1
            _, cols = columns(u)
            part_copy(0, u).wait_recv()
            psend[0, a, cols] = (psend[0, a, cols].astype(f32) + pass_y[:, cols].astype(f32)).astype(bf16)
            part_copy(4, u).start()
            part_copy(1, u).wait_recv()
            psend[1, b, cols] = (psend[1, b, cols].astype(f32) + pass_x[:, cols].astype(f32)).astype(bf16)
            part_copy(5, u).start()

        @pl.when(t >= 2)
        def _():
            u = t - 2
            d, cols = columns(u)
            for i in (2, 3, 4, 5):
                part_copy(i, u).wait_recv()
            feed = pown[:, cols] + sum_x[:, cols].astype(f32) + sum_y[:, cols].astype(f32)
            outv[:, cols] = (mid[:, cols].astype(f32) + feed).astype(bf16)
            pltpu.make_async_copy(outv.at[:, cols], out.at[:, cols], o_s.at[d]).start()

        return carry

    lax.fori_loop(0, np_ + 2, down_step, 0)

    for k in range(2):
        cross[k].wait_send()
        for part in range(2):
            for side in range(2):
                @pl.when((z < nz - 1) if side else (z > 0))
                def _():
                    to_side(k, part, side).wait_send()
            for s in range(nz):
                j = L.piece(s)
                to_core(k, j, part).wait_send()
                if s:
                    @pl.when(inner)
                    def _():
                        onward(k, j, part).wait_send()
    for cp in [wo_x, wo_c, relay, swap, back] + head_sends + [act_copy(i) for i in range(6)]:
        cp.wait_send()
    for zz in range(1, nz):
        @pl.when(z < zz)
        def _():
            hand_on(zz).wait_send()
    for t in range(np_):
        for i in range(6):
            part_copy(i, t).wait_send()
        d, cols = columns(t)
        pltpu.make_async_copy(outv.at[:, cols], out.at[:, cols], o_s.at[d]).wait()


def fused(
    n_sp, n_tp, stream, query, key, value, gate, rates, head_gain, out_w, mix_gain, up_w, down_w
):
    f32, bf16 = jnp.float32, jnp.bfloat16
    rows, width = stream.shape
    n_heads = query.shape[1] // KEY_CHANNELS
    half = up_w.shape[1] // 2
    nz, np_ = n_sp // 2, n_sp
    K = KEY_CHANNELS
    V, D = pltpu.VMEM, pltpu.SemaphoreType.DMA
    hbm = pl.BlockSpec(memory_space=pltpu.HBM)
    vmem = pl.BlockSpec(memory_space=pltpu.VMEM)
    return pl.pallas_call(
        functools.partial(layer_kernel, n_sp, n_tp),
        out_shape=jax.ShapeDtypeStruct((rows, width), bf16),
        in_specs=[hbm] * 6 + [vmem] * 2 + [hbm] * 3,
        out_specs=hbm,
        scratch_shapes=[
            V((2, width, half), bf16), V((2, width, half), bf16), V((n_tp, out_w.shape[0], width), bf16),
            V(query.shape, bf16), V(key.shape, bf16), V(value.shape, bf16), V(gate.shape, bf16), V(rates.shape, f32),
            V(value.shape, f32), V(query.shape, bf16), V((n_heads, DV, K), f32), V((n_heads, 1, K), f32),
            V((n_heads, DV + 16, K), bf16), V((DV + 16, K), bf16), V((DV + 16, K), bf16), V((nz, DV + 16, K), bf16),
            V((DV, K), f32), V((DV, K), bf16), V((n_heads, DV, K), bf16),
            V((n_tp, rows, value.shape[1]), bf16), V((n_tp, rows, value.shape[1]), bf16),
            V((4, rows, width), bf16), V((4, rows, 2 * half), bf16), V((rows, width), bf16),
            V((3, rows, width), bf16), V((rows, width), f32), V((rows, width), bf16), V((rows, width), bf16),
            V((rows // 2, width), bf16), V((rows // 2, width), bf16), V((rows, width), bf16),
            D((9,)), D((2, 2, 2)), D((2, nz, 2)), D((2, nz, 2)), D((2,)), D((2,)), D((2, nz, 2)), D((2, nz, 2)),
            D((3,)), D((3,)), D((2,)), D((2,)), D((nz,)), D((nz,)), D((3,)), D((3,)), D((6,)), D((6,)),
            D((6, np_)), D((6, np_)), D((np_,)),
        ],
        compiler_params=pltpu.CompilerParams(
            collective_id=0, has_side_effects=True, vmem_limit_bytes=67_000_000
        ),
        name="layer",
    )(stream, query, key, value, gate, rates, head_gain.reshape(1, -1), mix_gain.reshape(1, -1), out_w, up_w, down_w)


def solution(mesh):
    placed = (
        P(("sp", "tp"), None),
        P("sp", "tp"),
        P("sp", "tp"),
        P("sp", "tp"),
        P("sp", "tp"),
        P("sp", "tp"),
        P(),
        P("tp", None),
        P(),
        P("sp", "tp"),
        P("sp", "tp"),
    )

    def body(*args):
        return local(mesh.shape["sp"], mesh.shape["tp"], *args)

    if mesh.shape["tp"] == 4 and mesh.shape["sp"] % 2 == 0:
        def whole(*args):
            return fused(mesh.shape["sp"], mesh.shape["tp"], *args)

        return jax.shard_map(whole, mesh=mesh, in_specs=placed, out_specs=P(("sp", "tp"), None), check_vma=False)
    return jax.shard_map(body, mesh=mesh, in_specs=placed, out_specs=P(("sp", "tp"), None), check_vma=False)
```

```python
import functools

import jax
import jax.numpy as jnp
from jax import lax
from jax.experimental import pallas as pl
from jax.experimental.pallas import tpu as pltpu
from jax.sharding import PartitionSpec as P


KEY_CHANNELS = 128
DV = 256
BLOCK = 64
EPS = 1e-06


NT = (((1,), (1,)), ((), ()))
TN = (((0,), (0,)), ((), ()))


def local_states(q_ref, k_ref, v_ref, ld_ref, out_ref, qd_ref, state_ref):
    count = q_ref.shape[0] // BLOCK
    row = lax.broadcasted_iota(jnp.int32, (BLOCK, BLOCK), 0)
    col = lax.broadcasted_iota(jnp.int32, (BLOCK, BLOCK), 1)
    later = (col > row).astype(jnp.float32)
    scale = KEY_CHANNELS ** (-0.5)
    state = jnp.zeros((DV, KEY_CHANNELS), jnp.float32)
    total = jnp.zeros((1, KEY_CHANNELS), jnp.float32)
    for c in range(count):
        rows = pl.ds(c * BLOCK, BLOCK)
        rates = ld_ref[rows, :]
        rest = jnp.dot(later, rates, precision=lax.Precision.HIGHEST, preferred_element_type=jnp.float32)
        last = jnp.sum(rates, axis=0, keepdims=True)
        keys = (k_ref[rows, :].astype(jnp.float32) * jnp.exp(rest)).astype(jnp.bfloat16)
        update = lax.dot_general(v_ref[rows, :], keys, TN, preferred_element_type=jnp.float32)
        state = state * jnp.exp(last) + update
        total = total + last
        q = q_ref[rows, :]
        out_ref[rows, :] = lax.dot_general(
            q, state.astype(jnp.bfloat16), NT, preferred_element_type=jnp.float32
        ) * scale
        qd_ref[rows, :] = (q.astype(jnp.float32) * (jnp.exp(total) * scale)).astype(jnp.bfloat16)
    state_ref[0, :DV, :] = state.astype(jnp.bfloat16)
    state_ref[0, DV:, :] = jnp.broadcast_to(jnp.exp(total), (16, KEY_CHANNELS)).astype(jnp.bfloat16)


def finish_heads(own_ref, qd_ref, state_ref, gate_ref, gain_ref, out_ref):
    readout = own_ref[...] + lax.dot_general(
        qd_ref[...], state_ref[0, :DV, :], NT, preferred_element_type=jnp.float32
    )
    scaled = readout * lax.rsqrt(jnp.mean(readout * readout, axis=-1, keepdims=True) + EPS)
    gates = gate_ref[...].astype(jnp.float32)
    out_ref[...] = (scaled * gain_ref[...] * (gates / (1.0 + jnp.exp(-gates)))).astype(jnp.bfloat16)


def attention_local(q, k, v, ld):
    rows = q.shape[0]
    heads = q.shape[1] // KEY_CHANNELS
    kb = pl.BlockSpec((rows, KEY_CHANNELS), lambda h: (0, h))
    vb = pl.BlockSpec((rows, DV), lambda h: (0, h))
    return pl.pallas_call(
        local_states,
        grid=(heads,),
        in_specs=[kb, kb, vb, kb],
        out_specs=[vb, kb, pl.BlockSpec((1, DV + 16, KEY_CHANNELS), lambda h: (h, 0, 0))],
        out_shape=[
            jax.ShapeDtypeStruct((rows, heads * DV), jnp.float32),
            jax.ShapeDtypeStruct((rows, heads * KEY_CHANNELS), jnp.bfloat16),
            jax.ShapeDtypeStruct((heads, DV + 16, KEY_CHANNELS), jnp.bfloat16),
        ],
        cost_estimate=pl.CostEstimate(flops=6_000_000_000, bytes_accessed=8_000_000, transcendentals=0),
        name="local_states",
    )(q, k, v, ld)


def attention_finish(own, qd, state, gates, gain):
    rows = own.shape[0]
    heads = own.shape[1] // DV
    tile = rows // 2
    vb = pl.BlockSpec((tile, DV), lambda h, r: (r, h))
    return pl.pallas_call(
        finish_heads,
        grid=(heads, rows // tile),
        in_specs=[
            vb,
            pl.BlockSpec((tile, KEY_CHANNELS), lambda h, r: (r, h)),
            pl.BlockSpec((1, DV + 16, KEY_CHANNELS), lambda h, r: (h, 0, 0)),
            vb,
            pl.BlockSpec((1, DV), lambda h, r: (0, 0)),
        ],
        out_specs=vb,
        out_shape=jax.ShapeDtypeStruct(own.shape, jnp.bfloat16),
        cost_estimate=pl.CostEstimate(flops=3_000_000_000, bytes_accessed=4_000_000, transcendentals=0),
        name="finish_heads",
    )(own, qd, state, gates, gain)


def join(earlier, later):
    e, f = earlier.astype(jnp.float32), later.astype(jnp.float32)
    decay = f[:, DV : DV + 1]
    return jnp.concatenate(
        [decay * e[:, :DV] + f[:, :DV], jnp.broadcast_to(decay * e[:, DV : DV + 1], e[:, DV:].shape)], axis=1
    ).astype(jnp.bfloat16)


def shifted(a, by, n):
    return lax.ppermute(a, "sp", [(i, i + by) for i in range(n - by)])


def cycle_of(n):
    return list(range(0, n, 2)) + list(range(n - 1 - n % 2, 0, -2))


class Ring:
    def __init__(self, piece, n):
        self.n, self.cyc, self.piece = n, cycle_of(n), piece
        self.fwd = [(self.cyc[i], self.cyc[(i + 1) % n]) for i in range(n)]
        self.bwd = [(b, a) for a, b in self.fwd]
        self.left = self.right = piece
        self.hops = n // 2

    def hop(self, h):
        left, right = self.left, self.right
        if h == self.hops:
            half = self.piece.shape[0] // 2
            left, right = left[:half], right[half:]
        self.left = lax.ppermute(left, "sp", self.fwd)
        self.right = lax.ppermute(right, "sp", self.bwd)
        if h == self.hops:
            return [jnp.concatenate([self.left, self.right], axis=0)]
        return [self.left, self.right]


def owner_of(n, h):
    cyc = cycle_of(n)
    place = [0] * n
    for i, d in enumerate(cyc):
        place[d] = i
    me = jnp.asarray(place, jnp.int32)[lax.axis_index("sp")]
    cyc = jnp.asarray(cyc, jnp.int32)
    if h == 0:
        return [cyc[me]]
    back = cyc[(me - h) % n]
    return [back] if 2 * h == n else [back, cyc[(me + h) % n]]


def local(
    n_sp, n_tp, stream, query_rows, key_rows, value_rows, gate_rows, log_decay, head_gain, out_weight, mix_gain,
    up_weight, down_weight,
):
    nx = n_tp // 2
    own_rows = stream.shape[0]
    me = lax.axis_index("tp")
    x, core = me // 2, me % 2

    def across(a, dx):
        return lax.ppermute(a, "tp", [(((i // 2 + dx) % nx) * 2 + i % 2, i) for i in range(n_tp)])

    def swap(a):
        return lax.ppermute(a, "tp", [(i ^ 1, i) for i in range(n_tp)])

    up = Ring(up_weight, n_sp)
    down = Ring(down_weight, n_sp)
    width = up_weight.shape[0]
    up_full = lax.dynamic_update_slice_in_dim(
        jnp.zeros((width * n_sp, up_weight.shape[1]), up_weight.dtype), up_weight, owner_of(n_sp, 0)[0] * width, 0
    )
    ups = [up.hop(1)]
    downs = [[down_weight]]

    def tie(a, ring):
        a, ring.left, ring.right = lax.optimization_barrier((a, ring.left, ring.right))
        return a

    w = {(0, 0): out_weight}
    for dx in range(1, nx):
        w[dx, 0] = across(out_weight, dx)
    for dx in range(nx):
        w[dx, 1] = swap(w[dx, 0])

    own, qd, summary = attention_local(query_rows, key_rows, value_rows, log_decay)
    before, covered = tie(shifted(summary, 1, n_sp), up), 1
    while covered < n_sp - 1:
        wider = join(before, summary)
        if len(ups) < up.hops - 1:
            ups.append(up.hop(len(ups) + 1))
        before, covered = join(shifted(wider, covered + 1, n_sp), before), 2 * covered + 1
        before = tie(before, up)
    while len(ups) < up.hops:
        ups.append(up.hop(len(ups) + 1))
    before, down.left, down.right = lax.optimization_barrier((before, down.left, down.right))
    downs.append(down.hop(1))
    heads_out = attention_finish(own, qd, before, gate_rows, head_gain.reshape(1, DV))

    attn = None
    for dx in range(nx):
        for dc in range(2):
            to = ((x - dx) % nx) * 2 + (core + dc) % 2
            block = lax.dynamic_slice_in_dim(heads_out, to * own_rows, own_rows, 0)
            if (dx, dc) != (0, 0):
                block = lax.ppermute(
                    block, "tp", [(((i // 2 + dx) % nx) * 2 + (i % 2 + dc) % 2, i) for i in range(n_tp)]
                )
            term = jnp.dot(block, w[dx, dc], preferred_element_type=jnp.float32)
            attn = term if attn is None else attn + term
    midf = (stream.astype(jnp.float32) + attn).astype(jnp.bfloat16).astype(jnp.float32)
    normed = (
        midf * lax.rsqrt(jnp.mean(midf * midf, axis=-1, keepdims=True) + EPS) * mix_gain
    ).astype(jnp.bfloat16)

    normed = tie(normed, down)
    downs.append(down.hop(2))

    for h, pieces in enumerate(ups, 1):
        for piece, who in zip(pieces, owner_of(n_sp, h)):
            up_full = lax.dynamic_update_slice_in_dim(up_full, piece, who * width, 0)

    n = {(0, 0): normed}
    for dx in range(1, nx):
        n[dx, 0] = across(normed, dx)
    for dx in range(nx):
        n[dx, 1] = swap(n[dx, 0])
    n[nx - 1, 1] = tie(n[nx - 1, 1], down)
    while len(downs) <= down.hops:
        downs.append(down.hop(len(downs)))
    order = [(dx, dc) for dc in range(2) for dx in range(nx)]

    def hidden_of(rows):
        pre = jnp.dot(rows, up_full, preferred_element_type=jnp.float32)
        return jnp.square(jax.nn.relu(pre)).astype(jnp.bfloat16)

    hiddens = []
    for key in order:
        hiddens.append(hidden_of(n[key]))
    hidden = jnp.concatenate(hiddens, axis=0)

    out = jnp.zeros(stream.shape, jnp.bfloat16)
    mid = midf.astype(jnp.bfloat16)
    for h, pieces in enumerate(downs):
        whole = jnp.concatenate(pieces, axis=0) if len(pieces) > 1 else pieces[0]
        part = lax.dot_general(hidden, whole, NT, preferred_element_type=jnp.float32).astype(jnp.bfloat16)
        hidden, part = lax.optimization_barrier((hidden, part))
        half = nx * own_rows
        both = part[:half].astype(jnp.float32) + swap(part[half:]).astype(jnp.float32)
        feed = both[:own_rows]
        for dx in range(1, nx):
            send = both[dx * own_rows : (dx + 1) * own_rows].astype(jnp.bfloat16)
            feed = feed + across(send, nx - dx).astype(jnp.float32)
        for j, who in enumerate(owner_of(n_sp, h)):
            cols = lax.dynamic_slice_in_dim(mid, who * width, width, 1).astype(jnp.float32)
            done = (cols + feed[:, j * width : (j + 1) * width]).astype(jnp.bfloat16)
            out = lax.dynamic_update_slice_in_dim(out, done, who * width, 1)
    return out


UP_TILE = 512
CUT = 2
MESH = pl.DeviceIdType.MESH


class Links:
    def __init__(self, n_sp):
        self.sp, self.tp = lax.axis_index("sp"), lax.axis_index("tp")
        self.nz = n_sp // 2
        self.z, self.y = self.sp // 2, self.sp % 2
        self.x, self.c = self.tp // 2, self.tp % 2
        self.core = (self.sp, self.x * 2 + 1 - self.c)
        self.xn = (self.sp, (1 - self.x) * 2 + self.c)
        self.xo = (self.sp, (1 - self.x) * 2 + 1 - self.c)
        self.yn = (self.z * 2 + 1 - self.y, self.tp)

    def at_z(self, z):
        return (z * 2 + self.y, self.tp)

    def piece(self, s):
        z, n = self.z, self.nz
        near = jnp.minimum(z, n - 1 - z)
        turn = jnp.where(s % 2 == 1, z - (s + 1) // 2, z + s // 2)
        rest = jnp.where(z < n - 1 - z, s, n - 1 - s)
        return jnp.where(s <= 2 * near, turn, rest)


def remote(src, dst, send, recv, dev):
    return pltpu.make_async_remote_copy(
        src_ref=src, dst_ref=dst, send_sem=send, recv_sem=recv, device_id=dev, device_id_type=MESH
    )


def layer_kernel(
    n_sp, n_tp, stream, query, key, value, gate, rates_in, head_gain, mix_gain, out_w, up_w, down_w, out,
    up, down, wo, qv, kv, vv, gv, ldv, own, qd, state, total, summ, peer, tsend, trecv, prefix, bsend, before,
    heads, hrecv, acts, hidden, mid, psend, pown, sum_x, sum_y, pass_y, pass_x,
    ld_s, zown_s, zfwd_s, z_r, y_s, y_r, d_s, d_r, wo_s, wo_r, s_s, s_r, t_s, t_r, h_s, h_r, a_s, a_r, p_s, p_r,
):
    f32, bf16 = jnp.float32, jnp.bfloat16
    L = Links(n_sp)
    z, y, c, nz = L.z, L.y, L.c, L.nz
    rows, width = stream.shape
    span = query.shape[0]
    n_heads = query.shape[1] // KEY_CHANNELS
    slab, half = up_w.shape[0], up_w.shape[1] // 2
    half_rows = rows // 2
    fine = slab // CUT

    loads = [(query, qv), (key, kv), (value, vv), (rates_in, ldv)]
    first = [pltpu.make_async_copy(a, b, ld_s.at[i]) for i, (a, b) in enumerate(loads)]
    for cp in first:
        cp.start()
    barrier = pltpu.get_barrier_semaphore()
    partners = [L.core, L.xn, L.xo, L.yn]
    for dev in partners:
        pl.semaphore_signal(barrier, inc=1, device_id=dev, device_id_type=MESH)
    for has, to in ((z > 0, z - 1), (z < nz - 1, z + 1)):
        @pl.when(has)
        def _():
            pl.semaphore_signal(barrier, inc=1, device_id=L.at_z((to + nz) % nz), device_id_type=MESH)

    ends = jnp.where(z > 0, 1, 0) + jnp.where(z < nz - 1, 1, 0)
    pl.semaphore_wait(barrier, len(partners) + ends)

    bufs, source, cuts = (up, down), (up_w, down_w), (1, CUT)

    def place(kind, core, j, part, n=1):
        size = slab // cuts[kind]
        return bufs[kind].at[
            pl.ds(pl.multiple_of((j * 2 * cuts[kind] + part) * size, size), n * size),
            pl.ds(pl.multiple_of(core * half, half), half),
        ]

    def halfcols(kind, h, cut=None):
        size = slab // cuts[kind]
        return source[kind].at[pl.ds(0, slab) if cut is None else pl.ds(cut * size, size), pl.ds(pl.multiple_of(h * half, half), half)]

    def whole_part(kind, yy):
        return place(kind, c, z, yy * cuts[kind], cuts[kind])

    keep = [pltpu.make_async_copy(halfcols(k, y), whole_part(k, y), ld_s.at[6 + k]) for k in range(2)]
    cross = [remote(halfcols(k, 1 - y), whole_part(k, y), y_s.at[k], y_r.at[k], L.yn) for k in range(2)]

    def to_side(kind, far, cut, side):
        part = (1 - y if far else y) * cuts[kind] + cut
        src = place(kind, c, z, part) if far else halfcols(kind, y, cut)
        to = L.at_z((z + (1 if side else -1) + nz) % nz)
        return remote(src, place(kind, c, z, part), zown_s.at[kind, far, cut, side], z_r.at[kind, z, part], to)

    def to_core(kind, j, part, cut=None):
        dst = place(kind, c, j, part)
        src = dst if cut is None else halfcols(kind, y, cut)
        return remote(src, dst, d_s.at[kind, j, part], d_r.at[kind, j, part], L.core)

    def send_own(kind, far, sides=(0, 1)):
        for side in sides:
            @pl.when((z < nz - 1) if side else (z > 0))
            def _():
                for cut in range(cuts[kind]):
                    to_side(kind, far, cut, side).start()

    def share_own(kind, far):
        for cut in range(cuts[kind]):
            to_core(kind, z, (1 - y if far else y) * cuts[kind] + cut, None if far else cut).start()

    def onward(kind, j, part):
        to = jnp.where(j < z, z + 1, z - 1)
        dst = place(kind, c, j, part)
        return remote(dst, dst, zfwd_s.at[kind, j, part], z_r.at[kind, j, part], L.at_z((to + nz) % nz))

    inner = jnp.logical_and(z > 0, z < nz - 1)
    edge = jnp.logical_or(z == 0, z == nz - 1)

    def arrive(kind, s, part, forward):
        j = L.piece(s)
        cp = onward(kind, j, part)
        cp.wait_recv()
        if forward:
            cp.start()
        to_core(kind, j, part).start()

    def forward_inner(kind, s, part):
        @pl.when(inner)
        def _():
            arrive(kind, s, part, True)

    def arrive_edge(kind, s, part):
        @pl.when(edge)
        def _():
            arrive(kind, s, part, False)

    def from_core(kind, j, part):
        dst = place(kind, 1 - c, j, part)
        return remote(dst, dst, d_s.at[kind, j, part], d_r.at[kind, j, part], L.core)

    send_own(0, 0)
    send_own(1, 0, (0,))
    wo_half, wo_quarter = out_w.shape[0] // 2, out_w.shape[0] // 4

    def wo_rows(k):
        return pl.ds(0, wo_half) if k is None else pl.ds(pl.multiple_of(wo_half + k * wo_quarter, wo_quarter), wo_quarter)

    wo_own = pltpu.make_async_copy(out_w, wo.at[L.tp], ld_s.at[4])
    wo_c = remote(out_w, wo.at[L.tp], wo_s.at[1], wo_r.at[1], L.core)
    wo_b = remote(out_w.at[wo_rows(y), :], wo.at[L.tp, wo_rows(y), :], wo_s.at[3], wo_r.at[3], L.xn)
    wo_a = remote(out_w.at[wo_rows(None), :], wo.at[L.tp, wo_rows(None), :], wo_s.at[0], wo_r.at[0], L.xn)

    def wo_pass(k):
        ref = wo.at[L.xn[1], wo_rows(k), :]
        return remote(ref, ref, wo_s.at[4], wo_r.at[4], L.yn)

    wo_b.start()
    wo_a.start()
    wo_c.start()
    wo_own.start()
    for k in range(2):
        keep[k].start()
        share_own(k, 0)
    late = [pltpu.make_async_copy(gate, gv, ld_s.at[5]), pltpu.make_async_copy(stream, mid, ld_s.at[8])]
    for cp in late:
        cp.start()

    row = lax.broadcasted_iota(jnp.int32, (BLOCK, BLOCK), 0)
    col = lax.broadcasted_iota(jnp.int32, (BLOCK, BLOCK), 1)
    later = (col > row).astype(f32)
    scale = KEY_CHANNELS ** (-0.5)
    state[...] = jnp.zeros_like(state)
    total[...] = jnp.zeros_like(total)
    for cp in first:
        cp.wait()

    def block(i, carry):
        at = pl.ds(pl.multiple_of(i * BLOCK, BLOCK), BLOCK)
        for h in range(n_heads):
            ks, vs = pl.ds(h * KEY_CHANNELS, KEY_CHANNELS), pl.ds(h * DV, DV)
            rates = ldv[at, ks]
            rest = jnp.dot(later, rates, precision=lax.Precision.HIGHEST, preferred_element_type=f32)
            last = jnp.sum(rates, axis=0, keepdims=True)
            keys = (kv[at, ks].astype(f32) * jnp.exp(rest)).astype(bf16)
            update = lax.dot_general(vv[at, vs], keys, TN, preferred_element_type=f32)
            new = state[h] * jnp.exp(last) + update
            state[h] = new
            tot = total[h] + last
            total[h] = tot
            q = qv[at, ks]
            own[at, vs] = lax.dot_general(q, new.astype(bf16), NT, preferred_element_type=f32) * scale
            qd[at, ks] = (q.astype(f32) * (jnp.exp(tot) * scale)).astype(bf16)
        return carry

    lax.fori_loop(0, span // BLOCK, block, 0, unroll=4)
    for h in range(n_heads):
        summ[h, :DV, :] = state[h].astype(bf16)
        summ[h, DV:, :] = jnp.broadcast_to(jnp.exp(total[h]), (16, KEY_CHANNELS)).astype(bf16)

    swap = remote(summ.at[1 - y], peer, s_s.at[0], s_r.at[0], L.yn)
    swap.start()
    cross[0].start()
    swap.wait_recv()
    mine, other = summ[y].astype(f32), peer[...].astype(f32)
    is0 = y == 0
    early, late_ = jnp.where(is0, mine, other), jnp.where(is0, other, mine)
    dec = late_[DV : DV + 1]
    here = dec * early[:DV] + late_[:DV]
    onto_here = dec * early[DV : DV + 1]

    def hand_on(to):
        return remote(tsend, trecv, t_s.at[0], t_r.at[0], L.at_z((to + nz) % nz))

    @pl.when(z == nz - 2)
    def _():
        to_side(1, 0, 0, 1).start()

    prefix[...] = jnp.zeros_like(prefix)

    @pl.when(z > 0)
    def _():
        hand_on(z).wait_recv()
        prefix[...] = trecv[...].astype(f32)

    whole = prefix[...]

    @pl.when(z < nz - 1)
    def _():
        tsend[...] = (onto_here * whole + here).astype(bf16)
        hand_on(z + 1).start()
        for cut in range(1, CUT):
            to_side(1, 0, cut, 1).start()

    @pl.when(z < nz - 2)
    def _():
        to_side(1, 0, 0, 1).start()

    first_y = jnp.where(is0, mine, other)
    onto = first_y[DV : DV + 1] * whole + first_y[:DV]
    bsend[...] = jnp.where(is0, onto, whole).astype(bf16)
    before[y] = jnp.where(is0, whole, onto).astype(bf16)
    back = remote(bsend, before.at[y], s_s.at[1], s_r.at[1], L.yn)
    back.start()
    wo_from_b = remote(out_w.at[wo_rows(y), :], wo.at[L.xn[1], wo_rows(y), :], wo_s.at[3], wo_r.at[3], L.xn)
    wo_from_b.wait_recv()
    wo_pass(y).start()
    cross[1].start()
    cross[0].wait_recv()
    send_own(0, 1)
    share_own(0, 1)
    forward_inner(0, 1, y)
    forward_inner(0, 2, y)
    remote(bsend, before.at[1 - y], s_s.at[1], s_r.at[1], L.yn).wait_recv()
    late[0].wait()
    gain = head_gain[...]

    def finish(t):
        for r in range(0, rows, 128):
            at = pl.ds(pl.multiple_of(t * rows + r, 128), 128)
            for h in range(n_heads):
                ks, vs = pl.ds(h * KEY_CHANNELS, KEY_CHANNELS), pl.ds(h * DV, DV)
                readout = own[at, vs] + lax.dot_general(qd[at, ks], before[h], NT, preferred_element_type=f32)
                scaled = readout * lax.rsqrt(jnp.mean(readout * readout, axis=-1, keepdims=True) + EPS)
                g = gv[at, vs].astype(f32)
                heads[t, pl.ds(r, 128), vs] = (scaled * gain * (g / (1.0 + jnp.exp(-g)))).astype(bf16)

    head_sends = []
    for i, dev in enumerate((L.xn, L.xo, L.core)):
        t = dev[1]
        finish(t)
        cp = remote(heads.at[t], hrecv.at[L.tp], h_s.at[i], h_r.at[i], dev)
        cp.start()
        head_sends.append(cp)
    finish(L.tp)
    hrecv[L.tp] = heads[L.tp]
    forward_inner(0, 1, 1 - y)
    forward_inner(0, 2, 1 - y)

    remote(out_w.at[wo_rows(None), :], wo.at[L.xn[1], wo_rows(None), :], wo_s.at[0], wo_r.at[0], L.xn).wait_recv()
    wo_pass(1 - y).wait_recv()
    relay = remote(wo.at[L.xn[1]], wo.at[L.xn[1]], wo_s.at[2], wo_r.at[2], L.core)
    relay.start()
    remote(out_w, wo.at[L.core[1]], wo_s.at[1], wo_r.at[1], L.core).wait_recv()
    remote(wo.at[L.xo[1]], wo.at[L.xo[1]], wo_s.at[2], wo_r.at[2], L.core).wait_recv()
    wo_own.wait()
    late[1].wait()
    forward_inner(0, 3, y)
    arrive_edge(0, 1, y)
    arrive_edge(0, 1, 1 - y)
    for i, dev in enumerate((L.xn, L.xo, L.core)):
        remote(heads.at[dev[1]], hrecv.at[dev[1]], h_s.at[i], h_r.at[i], dev).wait_recv()

    square = jnp.zeros((rows, 1), f32)
    wide = min(512, width)
    for n in range(0, width, wide):
        cols = pl.ds(n, wide)
        acc = mid[:, cols].astype(f32)
        for t in range(n_tp):
            acc = acc + jnp.dot(hrecv[t], wo[t, :, cols], preferred_element_type=f32)
        m = acc.astype(bf16)
        mid[:, cols] = m
        m = m.astype(f32)
        square = square + jnp.sum(m * m, axis=-1, keepdims=True)
    norm = lax.rsqrt(square * (1.0 / width) + EPS)
    for n in range(0, width, wide):
        cols = pl.ds(n, wide)
        acts[:rows, cols] = (mid[:, cols].astype(f32) * norm * mix_gain[:, cols]).astype(bf16)

    a, b = pl.ds(0, half_rows), pl.ds(half_rows, half_rows)

    def act_copy(i):
        slot, part, dst, dev = [(0, 0, 1, L.xn), (0, 1, 1, L.xn), (0, 0, 2, L.yn), (0, 1, 2, L.yn), (1, 0, 3, L.yn), (2, 1, 3, L.xn)][i]
        src = acts.at[pl.ds(slot * rows + part * half_rows, half_rows), :]
        return remote(src, acts.at[pl.ds(dst * rows + part * half_rows, half_rows), :], a_s.at[i], a_r.at[i], dev)

    for i in (0, 3, 1, 2):
        act_copy(i).start()
    forward_inner(0, 3, 1 - y)
    cross[1].wait_recv()
    send_own(1, 1)
    share_own(1, 1)
    act_copy(0).wait_recv()
    act_copy(4).start()
    act_copy(3).wait_recv()
    act_copy(5).start()
    for s in (1, 2):
        for part in range(2 * CUT):
            forward_inner(1, s, part)
    arrive_edge(0, 2, y)
    arrive_edge(0, 2, 1 - y)
    for i in (1, 2, 4, 5):
        act_copy(i).wait_recv()
    for part in range(CUT):
        forward_inner(1, 3, part)

    arrive_edge(0, 3, y)
    arrive_edge(0, 3, 1 - y)
    keep[0].wait()
    for j in range(nz):
        for part in range(2):
            from_core(0, j, part).wait_recv()

    def up_step(n, carry):
        at = pl.ds(pl.multiple_of(n * UP_TILE, UP_TILE), UP_TILE)
        pre = jnp.maximum(jnp.dot(acts[...], up[:, at], preferred_element_type=f32), 0.0)
        hidden[:, at] = (pre * pre).astype(bf16)
        return carry

    lax.fori_loop(0, 2 * half // UP_TILE, up_step, 0)
    for part in range(CUT, 2 * CUT):
        forward_inner(1, 3, part)
    keep[1].wait()

    steps = 2 * nz * CUT
    final = steps - CUT

    def columns(u, n=1):
        d = (L.piece(u // (2 * CUT)) * 2 * CUT + u % (2 * CUT)) * fine
        return pl.ds(pl.multiple_of(d, fine), n * fine)

    def part_copy(i, u):
        cols = columns(u)
        src, dst, dev = [
            (psend.at[2, a, cols], pass_y.at[:, cols], L.yn),
            (psend.at[2, b, cols], pass_x.at[:, cols], L.xn),
            (psend.at[0, b, cols], sum_x.at[b, cols], L.xn),
            (psend.at[1, a, cols], sum_y.at[a, cols], L.yn),
            (psend.at[0, a, cols], sum_x.at[a, cols], L.xn),
            (psend.at[1, b, cols], sum_y.at[b, cols], L.yn),
        ][i]
        return remote(src, dst, p_s.at[i, u], p_r.at[i, u], dev)

    def terms_of(u, n):
        s = u // (2 * CUT)

        @pl.when(jnp.logical_and(edge, s > 0))
        def _():
            for k in range(n):
                arrive(1, s, u % (2 * CUT) + k, False)

        for k in range(n):
            from_core(1, L.piece(s), u % (2 * CUT) + k).wait_recv()
        cols = columns(u, n)
        terms = lax.dot_general(hidden[...], down[cols, :], NT, preferred_element_type=f32)
        pown[:, cols] = terms[:rows]
        for i in range(3):
            psend[i, :, cols] = terms[(i + 1) * rows : (i + 2) * rows].astype(bf16)
        for i in range(4):
            for k in range(n):
                part_copy(i, u + k).start()

    def pass_on(u):
        cols = columns(u)
        part_copy(0, u).wait_recv()
        psend[0, a, cols] = (psend[0, a, cols].astype(f32) + pass_y[:, cols].astype(f32)).astype(bf16)
        part_copy(4, u).start()
        part_copy(1, u).wait_recv()
        psend[1, b, cols] = (psend[1, b, cols].astype(f32) + pass_x[:, cols].astype(f32)).astype(bf16)
        part_copy(5, u).start()

    def close(u):
        cols = columns(u)
        for i in (2, 3, 4, 5):
            part_copy(i, u).wait_recv()
        feed = pown[:, cols] + sum_x[:, cols].astype(f32) + sum_y[:, cols].astype(f32)
        out[:, cols] = (mid[:, cols].astype(f32) + feed).astype(bf16)

    def down_step(u, carry):
        @pl.when(jnp.logical_and(u < final, u % CUT == 0))
        def _():
            terms_of(u, CUT)

        @pl.when(jnp.logical_and(u >= final, u < steps))
        def _():
            terms_of(u, 1)

        @pl.when(jnp.logical_and(u >= CUT, u < steps + CUT))
        def _():
            pass_on(u - CUT)

        @pl.when(u >= 2 * CUT)
        def _():
            close(u - 2 * CUT)

        return carry

    lax.fori_loop(0, steps + 2 * CUT, down_step, 0)

    for k in range(2):
        cross[k].wait_send()
        for far in range(2):
            for side in range(2):
                @pl.when((z < nz - 1) if side else (z > 0))
                def _():
                    for cut in range(cuts[k]):
                        to_side(k, far, cut, side).wait_send()
        for part in range(2 * cuts[k]):
            for s in range(nz):
                j = L.piece(s)
                to_core(k, j, part).wait_send()
                if s:
                    @pl.when(inner)
                    def _():
                        onward(k, j, part).wait_send()
    for cp in [wo_a, wo_b, wo_c, wo_pass(y), relay, swap, back] + head_sends + [act_copy(i) for i in range(6)]:
        cp.wait_send()

    @pl.when(z < nz - 1)
    def _():
        hand_on(z + 1).wait_send()

    for u in range(steps):
        for i in range(6):
            part_copy(i, u).wait_send()


def fused(
    n_sp, n_tp, stream, query, key, value, gate, rates, head_gain, out_w, mix_gain, up_w, down_w
):
    f32, bf16 = jnp.float32, jnp.bfloat16
    rows, width = stream.shape
    n_heads = query.shape[1] // KEY_CHANNELS
    half = up_w.shape[1] // 2
    nz, np_ = n_sp // 2, n_sp * CUT
    K = KEY_CHANNELS
    V, D = pltpu.VMEM, pltpu.SemaphoreType.DMA
    hbm = pl.BlockSpec(memory_space=pltpu.HBM)
    vmem = pl.BlockSpec(memory_space=pltpu.VMEM)
    return pl.pallas_call(
        functools.partial(layer_kernel, n_sp, n_tp),
        out_shape=pltpu.VMEM((rows, width), bf16),
        in_specs=[hbm] * 6 + [vmem] * 2 + [hbm] * 3,
        out_specs=vmem,
        scratch_shapes=[
            V((width, 2 * half), bf16), V((width, 2 * half), bf16), V((n_tp, out_w.shape[0], width), bf16),
            V(query.shape, bf16), V(key.shape, bf16), V(value.shape, bf16), V(gate.shape, bf16), V(rates.shape, f32),
            V(value.shape, f32), V(query.shape, bf16), V((n_heads, DV, K), f32), V((n_heads, 1, K), f32),
            V((n_heads, DV + 16, K), bf16), V((DV + 16, K), bf16), V((DV, K), bf16), V((DV, K), bf16),
            V((DV, K), f32), V((DV, K), bf16), V((n_heads, DV, K), bf16),
            V((n_tp, rows, value.shape[1]), bf16), V((n_tp, rows, value.shape[1]), bf16),
            V((4 * rows, width), bf16), V((4 * rows, 2 * half), bf16), V((rows, width), bf16),
            V((3, rows, width), bf16), V((rows, width), f32), V((rows, width), bf16), V((rows, width), bf16),
            V((rows // 2, width), bf16), V((rows // 2, width), bf16),
            D((9,)), D((2, 2, CUT, 2)), D((2, nz, 2 * CUT)), D((2, nz, 2 * CUT)), D((2,)), D((2,)), D((2, nz, 2 * CUT)),
            D((2, nz, 2 * CUT)),
            D((5,)), D((5,)), D((2,)), D((2,)), D((1,)), D((1,)), D((3,)), D((3,)), D((6,)), D((6,)),
            D((6, np_)), D((6, np_)),
        ],
        compiler_params=pltpu.CompilerParams(
            collective_id=0, has_side_effects=True, vmem_limit_bytes=58_000_000
        ),
        name="layer",
    )(stream, query, key, value, gate, rates, head_gain.reshape(1, -1), mix_gain.reshape(1, -1), out_w, up_w, down_w)


def solution(mesh):
    placed = (
        P(("sp", "tp"), None),
        P("sp", "tp"),
        P("sp", "tp"),
        P("sp", "tp"),
        P("sp", "tp"),
        P("sp", "tp"),
        P(),
        P("tp", None),
        P(),
        P("sp", "tp"),
        P("sp", "tp"),
    )

    def body(*args):
        return local(mesh.shape["sp"], mesh.shape["tp"], *args)

    if mesh.shape["tp"] == 4 and mesh.shape["sp"] % 2 == 0:
        def whole(*args):
            return fused(mesh.shape["sp"], mesh.shape["tp"], *args)

        return jax.shard_map(whole, mesh=mesh, in_specs=placed, out_specs=P(("sp", "tp"), None), check_vma=False)
    return jax.shard_map(body, mesh=mesh, in_specs=placed, out_specs=P(("sp", "tp"), None), check_vma=False)
```

```python
import functools

import jax
import jax.numpy as jnp
from jax import lax
from jax.experimental import pallas as pl
from jax.experimental.pallas import tpu as pltpu
from jax.sharding import PartitionSpec as P


KEY_CHANNELS = 128
DV = 256
BLOCK = 64
EPS = 1e-06


NT = (((1,), (1,)), ((), ()))
TN = (((0,), (0,)), ((), ()))


def local_states(q_ref, k_ref, v_ref, ld_ref, out_ref, qd_ref, state_ref):
    count = q_ref.shape[0] // BLOCK
    row = lax.broadcasted_iota(jnp.int32, (BLOCK, BLOCK), 0)
    col = lax.broadcasted_iota(jnp.int32, (BLOCK, BLOCK), 1)
    later = (col > row).astype(jnp.float32)
    scale = KEY_CHANNELS ** (-0.5)
    state = jnp.zeros((DV, KEY_CHANNELS), jnp.float32)
    total = jnp.zeros((1, KEY_CHANNELS), jnp.float32)
    for c in range(count):
        rows = pl.ds(c * BLOCK, BLOCK)
        rates = ld_ref[rows, :]
        rest = jnp.dot(later, rates, precision=lax.Precision.HIGHEST, preferred_element_type=jnp.float32)
        last = jnp.sum(rates, axis=0, keepdims=True)
        keys = (k_ref[rows, :].astype(jnp.float32) * jnp.exp(rest)).astype(jnp.bfloat16)
        update = lax.dot_general(v_ref[rows, :], keys, TN, preferred_element_type=jnp.float32)
        state = state * jnp.exp(last) + update
        total = total + last
        q = q_ref[rows, :]
        out_ref[rows, :] = lax.dot_general(
            q, state.astype(jnp.bfloat16), NT, preferred_element_type=jnp.float32
        ) * scale
        qd_ref[rows, :] = (q.astype(jnp.float32) * (jnp.exp(total) * scale)).astype(jnp.bfloat16)
    state_ref[0, :DV, :] = state.astype(jnp.bfloat16)
    state_ref[0, DV:, :] = jnp.broadcast_to(jnp.exp(total), (16, KEY_CHANNELS)).astype(jnp.bfloat16)


def finish_heads(own_ref, qd_ref, state_ref, gate_ref, gain_ref, out_ref):
    readout = own_ref[...] + lax.dot_general(
        qd_ref[...], state_ref[0, :DV, :], NT, preferred_element_type=jnp.float32
    )
    scaled = readout * lax.rsqrt(jnp.mean(readout * readout, axis=-1, keepdims=True) + EPS)
    gates = gate_ref[...].astype(jnp.float32)
    out_ref[...] = (scaled * gain_ref[...] * (gates / (1.0 + jnp.exp(-gates)))).astype(jnp.bfloat16)


def attention_local(q, k, v, ld):
    rows = q.shape[0]
    heads = q.shape[1] // KEY_CHANNELS
    kb = pl.BlockSpec((rows, KEY_CHANNELS), lambda h: (0, h))
    vb = pl.BlockSpec((rows, DV), lambda h: (0, h))
    return pl.pallas_call(
        local_states,
        grid=(heads,),
        in_specs=[kb, kb, vb, kb],
        out_specs=[vb, kb, pl.BlockSpec((1, DV + 16, KEY_CHANNELS), lambda h: (h, 0, 0))],
        out_shape=[
            jax.ShapeDtypeStruct((rows, heads * DV), jnp.float32),
            jax.ShapeDtypeStruct((rows, heads * KEY_CHANNELS), jnp.bfloat16),
            jax.ShapeDtypeStruct((heads, DV + 16, KEY_CHANNELS), jnp.bfloat16),
        ],
        cost_estimate=pl.CostEstimate(flops=6_000_000_000, bytes_accessed=8_000_000, transcendentals=0),
        name="local_states",
    )(q, k, v, ld)


def attention_finish(own, qd, state, gates, gain):
    rows = own.shape[0]
    heads = own.shape[1] // DV
    tile = rows // 2
    vb = pl.BlockSpec((tile, DV), lambda h, r: (r, h))
    return pl.pallas_call(
        finish_heads,
        grid=(heads, rows // tile),
        in_specs=[
            vb,
            pl.BlockSpec((tile, KEY_CHANNELS), lambda h, r: (r, h)),
            pl.BlockSpec((1, DV + 16, KEY_CHANNELS), lambda h, r: (h, 0, 0)),
            vb,
            pl.BlockSpec((1, DV), lambda h, r: (0, 0)),
        ],
        out_specs=vb,
        out_shape=jax.ShapeDtypeStruct(own.shape, jnp.bfloat16),
        cost_estimate=pl.CostEstimate(flops=3_000_000_000, bytes_accessed=4_000_000, transcendentals=0),
        name="finish_heads",
    )(own, qd, state, gates, gain)


def join(earlier, later):
    e, f = earlier.astype(jnp.float32), later.astype(jnp.float32)
    decay = f[:, DV : DV + 1]
    return jnp.concatenate(
        [decay * e[:, :DV] + f[:, :DV], jnp.broadcast_to(decay * e[:, DV : DV + 1], e[:, DV:].shape)], axis=1
    ).astype(jnp.bfloat16)


def shifted(a, by, n):
    return lax.ppermute(a, "sp", [(i, i + by) for i in range(n - by)])


def cycle_of(n):
    return list(range(0, n, 2)) + list(range(n - 1 - n % 2, 0, -2))


class Ring:
    def __init__(self, piece, n):
        self.n, self.cyc, self.piece = n, cycle_of(n), piece
        self.fwd = [(self.cyc[i], self.cyc[(i + 1) % n]) for i in range(n)]
        self.bwd = [(b, a) for a, b in self.fwd]
        self.left = self.right = piece
        self.hops = n // 2

    def hop(self, h):
        left, right = self.left, self.right
        if h == self.hops:
            half = self.piece.shape[0] // 2
            left, right = left[:half], right[half:]
        self.left = lax.ppermute(left, "sp", self.fwd)
        self.right = lax.ppermute(right, "sp", self.bwd)
        if h == self.hops:
            return [jnp.concatenate([self.left, self.right], axis=0)]
        return [self.left, self.right]


def owner_of(n, h):
    cyc = cycle_of(n)
    place = [0] * n
    for i, d in enumerate(cyc):
        place[d] = i
    me = jnp.asarray(place, jnp.int32)[lax.axis_index("sp")]
    cyc = jnp.asarray(cyc, jnp.int32)
    if h == 0:
        return [cyc[me]]
    back = cyc[(me - h) % n]
    return [back] if 2 * h == n else [back, cyc[(me + h) % n]]


def local(
    n_sp, n_tp, stream, query_rows, key_rows, value_rows, gate_rows, log_decay, head_gain, out_weight, mix_gain,
    up_weight, down_weight,
):
    nx = n_tp // 2
    own_rows = stream.shape[0]
    me = lax.axis_index("tp")
    x, core = me // 2, me % 2

    def across(a, dx):
        return lax.ppermute(a, "tp", [(((i // 2 + dx) % nx) * 2 + i % 2, i) for i in range(n_tp)])

    def swap(a):
        return lax.ppermute(a, "tp", [(i ^ 1, i) for i in range(n_tp)])

    up = Ring(up_weight, n_sp)
    down = Ring(down_weight, n_sp)
    width = up_weight.shape[0]
    up_full = lax.dynamic_update_slice_in_dim(
        jnp.zeros((width * n_sp, up_weight.shape[1]), up_weight.dtype), up_weight, owner_of(n_sp, 0)[0] * width, 0
    )
    ups = [up.hop(1)]
    downs = [[down_weight]]

    def tie(a, ring):
        a, ring.left, ring.right = lax.optimization_barrier((a, ring.left, ring.right))
        return a

    w = {(0, 0): out_weight}
    for dx in range(1, nx):
        w[dx, 0] = across(out_weight, dx)
    for dx in range(nx):
        w[dx, 1] = swap(w[dx, 0])

    own, qd, summary = attention_local(query_rows, key_rows, value_rows, log_decay)
    before, covered = tie(shifted(summary, 1, n_sp), up), 1
    while covered < n_sp - 1:
        wider = join(before, summary)
        if len(ups) < up.hops - 1:
            ups.append(up.hop(len(ups) + 1))
        before, covered = join(shifted(wider, covered + 1, n_sp), before), 2 * covered + 1
        before = tie(before, up)
    while len(ups) < up.hops:
        ups.append(up.hop(len(ups) + 1))
    before, down.left, down.right = lax.optimization_barrier((before, down.left, down.right))
    downs.append(down.hop(1))
    heads_out = attention_finish(own, qd, before, gate_rows, head_gain.reshape(1, DV))

    attn = None
    for dx in range(nx):
        for dc in range(2):
            to = ((x - dx) % nx) * 2 + (core + dc) % 2
            block = lax.dynamic_slice_in_dim(heads_out, to * own_rows, own_rows, 0)
            if (dx, dc) != (0, 0):
                block = lax.ppermute(
                    block, "tp", [(((i // 2 + dx) % nx) * 2 + (i % 2 + dc) % 2, i) for i in range(n_tp)]
                )
            term = jnp.dot(block, w[dx, dc], preferred_element_type=jnp.float32)
            attn = term if attn is None else attn + term
    midf = (stream.astype(jnp.float32) + attn).astype(jnp.bfloat16).astype(jnp.float32)
    normed = (
        midf * lax.rsqrt(jnp.mean(midf * midf, axis=-1, keepdims=True) + EPS) * mix_gain
    ).astype(jnp.bfloat16)

    normed = tie(normed, down)
    downs.append(down.hop(2))

    for h, pieces in enumerate(ups, 1):
        for piece, who in zip(pieces, owner_of(n_sp, h)):
            up_full = lax.dynamic_update_slice_in_dim(up_full, piece, who * width, 0)

    n = {(0, 0): normed}
    for dx in range(1, nx):
        n[dx, 0] = across(normed, dx)
    for dx in range(nx):
        n[dx, 1] = swap(n[dx, 0])
    n[nx - 1, 1] = tie(n[nx - 1, 1], down)
    while len(downs) <= down.hops:
        downs.append(down.hop(len(downs)))
    order = [(dx, dc) for dc in range(2) for dx in range(nx)]

    def hidden_of(rows):
        pre = jnp.dot(rows, up_full, preferred_element_type=jnp.float32)
        return jnp.square(jax.nn.relu(pre)).astype(jnp.bfloat16)

    hiddens = []
    for key in order:
        hiddens.append(hidden_of(n[key]))
    hidden = jnp.concatenate(hiddens, axis=0)

    out = jnp.zeros(stream.shape, jnp.bfloat16)
    mid = midf.astype(jnp.bfloat16)
    for h, pieces in enumerate(downs):
        whole = jnp.concatenate(pieces, axis=0) if len(pieces) > 1 else pieces[0]
        part = lax.dot_general(hidden, whole, NT, preferred_element_type=jnp.float32).astype(jnp.bfloat16)
        hidden, part = lax.optimization_barrier((hidden, part))
        half = nx * own_rows
        both = part[:half].astype(jnp.float32) + swap(part[half:]).astype(jnp.float32)
        feed = both[:own_rows]
        for dx in range(1, nx):
            send = both[dx * own_rows : (dx + 1) * own_rows].astype(jnp.bfloat16)
            feed = feed + across(send, nx - dx).astype(jnp.float32)
        for j, who in enumerate(owner_of(n_sp, h)):
            cols = lax.dynamic_slice_in_dim(mid, who * width, width, 1).astype(jnp.float32)
            done = (cols + feed[:, j * width : (j + 1) * width]).astype(jnp.bfloat16)
            out = lax.dynamic_update_slice_in_dim(out, done, who * width, 1)
    return out


UP_TILE = 512
CUT = 2
MESH = pl.DeviceIdType.MESH


class Links:
    def __init__(self, n_sp):
        self.sp, self.tp = lax.axis_index("sp"), lax.axis_index("tp")
        self.nz = n_sp // 2
        self.z, self.y = self.sp // 2, self.sp % 2
        self.x, self.c = self.tp // 2, self.tp % 2
        self.core = (self.sp, self.x * 2 + 1 - self.c)
        self.xn = (self.sp, (1 - self.x) * 2 + self.c)
        self.xo = (self.sp, (1 - self.x) * 2 + 1 - self.c)
        self.yn = (self.z * 2 + 1 - self.y, self.tp)

    def at_z(self, z):
        return (z * 2 + self.y, self.tp)

    def piece(self, s):
        z, n = self.z, self.nz
        near = jnp.minimum(z, n - 1 - z)
        turn = jnp.where(s % 2 == 1, z - (s + 1) // 2, z + s // 2)
        rest = jnp.where(z < n - 1 - z, s, n - 1 - s)
        return jnp.where(s <= 2 * near, turn, rest)


def remote(src, dst, send, recv, dev):
    return pltpu.make_async_remote_copy(
        src_ref=src, dst_ref=dst, send_sem=send, recv_sem=recv, device_id=dev, device_id_type=MESH
    )


def layer_kernel(
    n_sp, n_tp, stream, query, key, value, gate, rates_in, head_gain, mix_gain, out_w, up_w, down_w, out,
    up, down, wo, qv, kv, vv, gv, ldv, own, qd, state, total, summ, peer, tsend, trecv, prefix, bsend, before,
    heads, hrecv, acts, hidden, mid, psend, pown, sum_x, sum_y, pass_y, pass_x,
    gain_h, gain_m, ld_s, zown_s, zfwd_s, z_r, y_s, y_r, d_s, du_r, dd_r, wo_s, wo_r, s_s, s_r, t_s, t_r, h_s, h_r, a_s, a_r,
    p_s, p_r,
):
    f32, bf16 = jnp.float32, jnp.bfloat16
    L = Links(n_sp)
    z, y, c, nz = L.z, L.y, L.c, L.nz
    rows, width = stream.shape
    span = query.shape[0]
    n_heads = query.shape[1] // KEY_CHANNELS
    slab, half = up_w.shape[0], up_w.shape[1] // 2
    half_rows = rows // 2
    fine = slab // CUT

    barrier = pltpu.get_barrier_semaphore()
    partners = [L.core, L.xn, L.xo, L.yn]
    for dev in partners:
        pl.semaphore_signal(barrier, inc=1, device_id=dev, device_id_type=MESH)
    for has, to in ((z > 0, z - 1), (z < nz - 1, z + 1)):
        @pl.when(has)
        def _():
            pl.semaphore_signal(barrier, inc=1, device_id=L.at_z((to + nz) % nz), device_id_type=MESH)

    loads = [(query, qv), (key, kv), (value, vv), (rates_in, ldv)]
    first = [pltpu.make_async_copy(a, b, ld_s.at[i]) for i, (a, b) in enumerate(loads)]
    for cp in first:
        cp.start()
    ends = jnp.where(z > 0, 1, 0) + jnp.where(z < nz - 1, 1, 0)
    pl.semaphore_wait(barrier, len(partners) + ends)

    bufs, source, cuts = (up, down), (up_w, down_w), (1, CUT)

    def place(kind, core, j, part, n=1):
        size = slab // cuts[kind]
        return bufs[kind].at[
            pl.ds(pl.multiple_of((j * 2 * cuts[kind] + part) * size, size), n * size),
            pl.ds(pl.multiple_of(core * half, half), half),
        ]

    def halfcols(kind, h, cut=None):
        size = slab // cuts[kind]
        return source[kind].at[pl.ds(0, slab) if cut is None else pl.ds(cut * size, size), pl.ds(pl.multiple_of(h * half, half), half)]

    def whole_part(kind, yy):
        return place(kind, c, z, yy * cuts[kind], cuts[kind])

    keep = [pltpu.make_async_copy(halfcols(k, y), whole_part(k, y), ld_s.at[6 + k]) for k in range(2)]
    cross = [remote(halfcols(k, 1 - y), whole_part(k, y), y_s.at[0], y_r.at[k], L.yn) for k in range(2)]

    def z_slot(kind, part):
        return part + 2 * kind

    def to_side(kind, far, cut, side):
        part = (1 - y if far else y) * cuts[kind] + cut
        src = place(kind, c, z, part) if far else halfcols(kind, y, cut)
        to = L.at_z((z + (1 if side else -1) + nz) % nz)
        return remote(src, place(kind, c, z, part), zown_s.at[side], z_r.at[z, z_slot(kind, part)], to)

    final = (2 * nz - 1) * CUT

    def core_r(kind, s, part):
        if kind == 0:
            return du_r.at[0]
        u = s * 2 * CUT + part
        return dd_r.at[jnp.where(u < final, u // CUT, final // CUT + u - final)]

    def to_core(kind, s, part, cut=None):
        dst = place(kind, c, L.piece(s), part)
        src = dst if cut is None else halfcols(kind, y, cut)
        return remote(src, dst, d_s.at[kind], core_r(kind, s, part), L.core)

    def send_own(kind, far, sides=(0, 1)):
        for side in sides:
            @pl.when((z < nz - 1) if side else (z > 0))
            def _():
                for cut in range(cuts[kind]):
                    to_side(kind, far, cut, side).start()

    def share_own(kind, far):
        for cut in range(cuts[kind]):
            to_core(kind, 0, (1 - y if far else y) * cuts[kind] + cut, None if far else cut).start()

    def onward(kind, j, part):
        to = jnp.where(j < z, z + 1, z - 1)
        dst = place(kind, c, j, part)
        return remote(dst, dst, zfwd_s.at[kind], z_r.at[j, z_slot(kind, part)], L.at_z((to + nz) % nz))

    inner = jnp.logical_and(z > 0, z < nz - 1)
    edge = jnp.logical_or(z == 0, z == nz - 1)

    def arrive(kind, s, part, forward):
        j = L.piece(s)
        cp = onward(kind, j, part)
        cp.wait_recv()
        if forward:
            cp.start()
        to_core(kind, s, part).start()

    def forward_inner(kind, s, part):
        @pl.when(inner)
        def _():
            arrive(kind, s, part, True)

    def arrive_edge(kind, s, part):
        @pl.when(edge)
        def _():
            arrive(kind, s, part, False)

    send_own(0, 0)
    send_own(1, 0, (0,))
    wo_half, wo_quarter = out_w.shape[0] // 2, out_w.shape[0] // 4

    def wo_rows(k):
        return pl.ds(0, wo_half) if k is None else pl.ds(pl.multiple_of(wo_half + k * wo_quarter, wo_quarter), wo_quarter)

    wo_own = pltpu.make_async_copy(out_w, wo.at[L.tp], ld_s.at[4])
    wo_c = remote(out_w, wo.at[L.tp], wo_s.at[0], wo_r.at[1], L.core)
    wo_b = remote(out_w.at[wo_rows(y), :], wo.at[L.tp, wo_rows(y), :], wo_s.at[0], wo_r.at[3], L.xn)
    wo_a = remote(out_w.at[wo_rows(None), :], wo.at[L.tp, wo_rows(None), :], wo_s.at[0], wo_r.at[0], L.xn)

    def wo_pass(k):
        ref = wo.at[L.xn[1], wo_rows(k), :]
        return remote(ref, ref, wo_s.at[0], wo_r.at[4], L.yn)

    wo_b.start()
    wo_a.start()
    wo_c.start()
    wo_own.start()
    for k in range(2):
        keep[k].start()
        share_own(k, 0)
    late = [pltpu.make_async_copy(gate, gv, ld_s.at[5]), pltpu.make_async_copy(stream, mid, ld_s.at[8])]
    late += [pltpu.make_async_copy(head_gain, gain_h, ld_s.at[9]), pltpu.make_async_copy(mix_gain, gain_m, ld_s.at[10])]
    for cp in late:
        cp.start()

    row = lax.broadcasted_iota(jnp.int32, (BLOCK, BLOCK), 0)
    col = lax.broadcasted_iota(jnp.int32, (BLOCK, BLOCK), 1)
    later = (col > row).astype(f32)
    scale = KEY_CHANNELS ** (-0.5)
    state[...] = jnp.zeros_like(state)
    total[...] = jnp.zeros_like(total)
    for cp in first:
        cp.wait()

    def block(i, carry):
        at = pl.ds(pl.multiple_of(i * BLOCK, BLOCK), BLOCK)
        for h in range(n_heads):
            ks, vs = pl.ds(h * KEY_CHANNELS, KEY_CHANNELS), pl.ds(h * DV, DV)
            rates = ldv[at, ks]
            rest = jnp.dot(later, rates, precision=lax.Precision.HIGHEST, preferred_element_type=f32)
            last = jnp.sum(rates, axis=0, keepdims=True)
            keys = (kv[at, ks].astype(f32) * jnp.exp(rest)).astype(bf16)
            update = lax.dot_general(vv[at, vs], keys, TN, preferred_element_type=f32)
            new = state[h] * jnp.exp(last) + update
            state[h] = new
            tot = total[h] + last
            total[h] = tot
            q = qv[at, ks]
            own[at, vs] = lax.dot_general(q, new.astype(bf16), NT, preferred_element_type=f32) * scale
            qd[at, ks] = (q.astype(f32) * (jnp.exp(tot) * scale)).astype(bf16)
        return carry

    lax.fori_loop(0, span // BLOCK, block, 0, unroll=4)
    for h in range(n_heads):
        summ[h, :DV, :] = state[h].astype(bf16)
        summ[h, DV:, :] = jnp.broadcast_to(jnp.exp(total[h]), (16, KEY_CHANNELS)).astype(bf16)

    swap = remote(summ.at[1 - y], peer, s_s.at[0], s_r.at[0], L.yn)
    swap.start()
    cross[0].start()
    swap.wait_recv()
    mine, other = summ[y].astype(f32), peer[...].astype(f32)
    is0 = y == 0
    early, late_ = jnp.where(is0, mine, other), jnp.where(is0, other, mine)
    dec = late_[DV : DV + 1]
    here = dec * early[:DV] + late_[:DV]
    onto_here = dec * early[DV : DV + 1]

    def hand_on(to):
        return remote(tsend, trecv, t_s.at[0], t_r.at[0], L.at_z((to + nz) % nz))

    @pl.when(z == nz - 2)
    def _():
        to_side(1, 0, 0, 1).start()

    prefix[...] = jnp.zeros_like(prefix)

    @pl.when(z > 0)
    def _():
        hand_on(z).wait_recv()
        prefix[...] = trecv[...].astype(f32)

    whole = prefix[...]

    @pl.when(z < nz - 1)
    def _():
        tsend[...] = (onto_here * whole + here).astype(bf16)
        hand_on(z + 1).start()
        for cut in range(1, CUT):
            to_side(1, 0, cut, 1).start()

    @pl.when(z < nz - 2)
    def _():
        to_side(1, 0, 0, 1).start()

    first_y = jnp.where(is0, mine, other)
    onto = first_y[DV : DV + 1] * whole + first_y[:DV]
    bsend[...] = jnp.where(is0, onto, whole).astype(bf16)
    before[y] = jnp.where(is0, whole, onto).astype(bf16)
    back = remote(bsend, before.at[y], s_s.at[1], s_r.at[1], L.yn)
    back.start()
    wo_from_b = remote(out_w.at[wo_rows(y), :], wo.at[L.xn[1], wo_rows(y), :], wo_s.at[0], wo_r.at[3], L.xn)
    wo_from_b.wait_recv()
    wo_pass(y).start()
    cross[1].start()
    cross[0].wait_recv()
    send_own(0, 1)
    share_own(0, 1)
    forward_inner(0, 1, y)
    forward_inner(0, 2, y)
    remote(bsend, before.at[1 - y], s_s.at[1], s_r.at[1], L.yn).wait_recv()
    late[0].wait()
    late[2].wait()
    gain = gain_h[...]

    def finish(t):
        for r in range(0, rows, 128):
            at = pl.ds(pl.multiple_of(t * rows + r, 128), 128)
            for h in range(n_heads):
                ks, vs = pl.ds(h * KEY_CHANNELS, KEY_CHANNELS), pl.ds(h * DV, DV)
                readout = own[at, vs] + lax.dot_general(qd[at, ks], before[h], NT, preferred_element_type=f32)
                scaled = readout * lax.rsqrt(jnp.mean(readout * readout, axis=-1, keepdims=True) + EPS)
                g = gv[at, vs].astype(f32)
                heads[t, pl.ds(r, 128), vs] = (scaled * gain * (g / (1.0 + jnp.exp(-g)))).astype(bf16)

    for dev in (L.xn, L.xo, L.core):
        t = dev[1]
        finish(t)
        cp = remote(heads.at[t], hrecv.at[L.tp], h_s.at[0], h_r.at[0], dev)
        cp.start()
    finish(L.tp)
    hrecv[L.tp] = heads[L.tp]
    forward_inner(0, 1, 1 - y)
    forward_inner(0, 2, 1 - y)

    remote(out_w.at[wo_rows(None), :], wo.at[L.xn[1], wo_rows(None), :], wo_s.at[0], wo_r.at[0], L.xn).wait_recv()
    wo_pass(1 - y).wait_recv()
    relay = remote(wo.at[L.xn[1]], wo.at[L.xn[1]], wo_s.at[0], wo_r.at[2], L.core)
    relay.start()
    remote(out_w, wo.at[L.core[1]], wo_s.at[0], wo_r.at[1], L.core).wait_recv()
    remote(wo.at[L.xo[1]], wo.at[L.xo[1]], wo_s.at[0], wo_r.at[2], L.core).wait_recv()
    wo_own.wait()
    late[1].wait()
    late[3].wait()
    forward_inner(0, 3, y)
    arrive_edge(0, 1, y)
    arrive_edge(0, 1, 1 - y)
    others = pl.ds(0, n_tp - 1)
    all_heads = remote(heads.at[others], hrecv.at[others], h_s.at[0], h_r.at[0], L.xn)
    all_heads.wait_recv()

    square = jnp.zeros((rows, 1), f32)
    wide = min(512, width)
    for n in range(0, width, wide):
        cols = pl.ds(n, wide)
        acc = mid[:, cols].astype(f32)
        for t in range(n_tp):
            acc = acc + jnp.dot(hrecv[t], wo[t, :, cols], preferred_element_type=f32)
        m = acc.astype(bf16)
        mid[:, cols] = m
        m = m.astype(f32)
        square = square + jnp.sum(m * m, axis=-1, keepdims=True)
    norm = lax.rsqrt(square * (1.0 / width) + EPS)
    for n in range(0, width, wide):
        cols = pl.ds(n, wide)
        acts[:rows, cols] = (mid[:, cols].astype(f32) * norm * gain_m[:, cols]).astype(bf16)

    a, b = pl.ds(0, half_rows), pl.ds(half_rows, half_rows)

    def act_copy(i):
        slot, part, dst, dev = [(0, 0, 1, L.xn), (0, 1, 1, L.xn), (0, 0, 2, L.yn), (0, 1, 2, L.yn), (1, 0, 3, L.yn), (2, 1, 3, L.xn)][i]
        src = acts.at[pl.ds(slot * rows + part * half_rows, half_rows), :]
        return remote(src, acts.at[pl.ds(dst * rows + part * half_rows, half_rows), :], a_s.at[0], a_r.at[i], dev)

    for i in (0, 3, 1, 2):
        act_copy(i).start()
    forward_inner(0, 3, 1 - y)
    cross[1].wait_recv()
    send_own(1, 1)
    share_own(1, 1)
    act_copy(0).wait_recv()
    act_copy(4).start()
    act_copy(3).wait_recv()
    act_copy(5).start()
    for s in (1, 2):
        for part in range(2 * CUT):
            forward_inner(1, s, part)
    arrive_edge(0, 2, y)
    arrive_edge(0, 2, 1 - y)
    for i in (1, 2, 4, 5):
        act_copy(i).wait_recv()
    for part in range(CUT):
        forward_inner(1, 3, part)

    arrive_edge(0, 3, y)
    arrive_edge(0, 3, 1 - y)
    keep[0].wait()
    theirs = up.at[:, pl.ds(pl.multiple_of((1 - c) * half, half), half)]
    remote(theirs, theirs, d_s.at[0], du_r.at[0], L.core).wait_recv()

    def up_step(n, carry):
        at = pl.ds(pl.multiple_of(n * UP_TILE, UP_TILE), UP_TILE)
        pre = jnp.maximum(jnp.dot(acts[...], up[:, at], preferred_element_type=f32), 0.0)
        hidden[:, at] = (pre * pre).astype(bf16)
        return carry

    lax.fori_loop(0, 2 * half // UP_TILE, up_step, 0)
    for part in range(CUT, 2 * CUT):
        forward_inner(1, 3, part)
    keep[1].wait()

    steps = 2 * nz * CUT

    def columns(u, n=1):
        d = (L.piece(u // (2 * CUT)) * 2 * CUT + u % (2 * CUT)) * fine
        return pl.ds(pl.multiple_of(d, fine), n * fine)

    def part_copy(i, u):
        cols = columns(u)
        src, dst, dev = [
            (psend.at[2, a, cols], pass_y.at[:, cols], L.yn),
            (psend.at[2, b, cols], pass_x.at[:, cols], L.xn),
            (psend.at[0, b, cols], sum_x.at[b, cols], L.xn),
            (psend.at[1, a, cols], sum_y.at[a, cols], L.yn),
            (psend.at[0, a, cols], sum_x.at[a, cols], L.xn),
            (psend.at[1, b, cols], sum_y.at[b, cols], L.yn),
        ][i]
        return remote(src, dst, p_s.at[0], p_r.at[0 if i < 2 else 1, u], dev)

    def terms_of(u, n):
        s = u // (2 * CUT)

        @pl.when(jnp.logical_and(edge, s > 0))
        def _():
            for k in range(n):
                arrive(1, s, u % (2 * CUT) + k, False)

        theirs = down.at[columns(u, n), pl.ds(pl.multiple_of((1 - c) * half, half), half)]
        remote(theirs, theirs, d_s.at[1], core_r(1, s, u % (2 * CUT)), L.core).wait_recv()
        cols = columns(u, n)
        terms = lax.dot_general(hidden[...], down[cols, :], NT, preferred_element_type=f32)
        pown[:, cols] = terms[:rows]
        for i in range(3):
            psend[i, :, cols] = terms[(i + 1) * rows : (i + 2) * rows].astype(bf16)
        for i in range(4):
            for k in range(n):
                part_copy(i, u + k).start()

    def pass_on(u):
        cols = columns(u)
        passed = psend.at[0, :, cols]
        remote(passed, passed, p_s.at[0], p_r.at[0, u], L.xn).wait_recv()
        psend[0, a, cols] = (psend[0, a, cols].astype(f32) + pass_y[:, cols].astype(f32)).astype(bf16)
        part_copy(4, u).start()
        psend[1, b, cols] = (psend[1, b, cols].astype(f32) + pass_x[:, cols].astype(f32)).astype(bf16)
        part_copy(5, u).start()

    def close(u):
        cols = columns(u)
        sums = psend.at[pl.ds(0, 2), :, cols]
        remote(sums, sums, p_s.at[0], p_r.at[1, u], L.xn).wait_recv()
        feed = pown[:, cols] + sum_x[:, cols].astype(f32) + sum_y[:, cols].astype(f32)
        out[:, cols] = (mid[:, cols].astype(f32) + feed).astype(bf16)

    def down_step(u, carry):
        @pl.when(jnp.logical_and(u < final, u % CUT == 0))
        def _():
            terms_of(u, CUT)

        @pl.when(jnp.logical_and(u >= final, u < steps))
        def _():
            terms_of(u, 1)

        @pl.when(jnp.logical_and(u >= CUT, u < steps + CUT))
        def _():
            pass_on(u - CUT)

        @pl.when(u >= 2 * CUT)
        def _():
            close(u - 2 * CUT)

        return carry

    lax.fori_loop(0, steps + 2 * CUT, down_step, 0)

    def sent(ref, sem):
        remote(ref, ref, sem, sem, L.core).wait_send()

    mine_cols = pl.ds(0, half)
    sent(up.at[pl.ds(0, 2 * slab), mine_cols], y_s.at[0])
    for side in range(2):
        @pl.when((z < nz - 1) if side else (z > 0))
        def _():
            sent(up.at[pl.ds(0, 4 * slab), mine_cols], zown_s.at[side])
    for k in range(2):
        sent(up.at[:, mine_cols], d_s.at[k])

        @pl.when(inner)
        def _():
            sent(up.at[pl.ds(0, 2 * slab * (nz - 1)), mine_cols], zfwd_s.at[k])
    sent(wo.at[pl.ds(0, 3)], wo_s.at[0])
    swap.wait_send()
    back.wait_send()

    @pl.when(z < nz - 1)
    def _():
        hand_on(z + 1).wait_send()

    all_heads.wait_send()
    sent(acts.at[pl.ds(0, 3 * rows), :], a_s.at[0])
    sent(psend, p_s.at[0])


def fused(
    n_sp, n_tp, stream, query, key, value, gate, rates, head_gain, out_w, mix_gain, up_w, down_w
):
    f32, bf16 = jnp.float32, jnp.bfloat16
    rows, width = stream.shape
    n_heads = query.shape[1] // KEY_CHANNELS
    half = up_w.shape[1] // 2
    nz, np_ = n_sp // 2, n_sp * CUT
    K = KEY_CHANNELS
    V, D = pltpu.VMEM, pltpu.SemaphoreType.DMA
    hbm = pl.BlockSpec(memory_space=pltpu.HBM)
    vmem = pl.BlockSpec(memory_space=pltpu.VMEM)
    return pl.pallas_call(
        functools.partial(layer_kernel, n_sp, n_tp),
        out_shape=pltpu.VMEM((rows, width), bf16),
        in_specs=[hbm] * 11,
        out_specs=vmem,
        scratch_shapes=[
            V((width, 2 * half), bf16), V((width, 2 * half), bf16), V((n_tp, out_w.shape[0], width), bf16),
            V(query.shape, bf16), V(key.shape, bf16), V(value.shape, bf16), V(gate.shape, bf16), V(rates.shape, f32),
            V(value.shape, f32), V(query.shape, bf16), V((n_heads, DV, K), f32), V((n_heads, 1, K), f32),
            V((n_heads, DV + 16, K), bf16), V((DV + 16, K), bf16), V((DV, K), bf16), V((DV, K), bf16),
            V((DV, K), f32), V((DV, K), bf16), V((n_heads, DV, K), bf16),
            V((n_tp, rows, value.shape[1]), bf16), V((n_tp, rows, value.shape[1]), bf16),
            V((4 * rows, width), bf16), V((4 * rows, 2 * half), bf16), V((rows, width), bf16),
            V((3, rows, width), bf16), V((rows, width), f32), V((rows, width), bf16), V((rows, width), bf16),
            V((rows // 2, width), bf16), V((rows // 2, width), bf16),
            V((1, head_gain.shape[0]), f32), V((1, width), f32),
            D((11,)), D((2,)), D((2,)), D((nz, 2 + 2 * CUT)), D((1,)), D((2,)), D((2,)), D((1,)), D((2 * nz - 1 + CUT,)),
            D((1,)), D((5,)), D((2,)), D((2,)), D((1,)), D((1,)), D((1,)), D((1,)), D((1,)), D((6,)), D((1,)), D((2, np_)),
        ],
        compiler_params=pltpu.CompilerParams(
            collective_id=0, has_side_effects=True, vmem_limit_bytes=58_000_000
        ),
        name="layer",
    )(stream, query, key, value, gate, rates, head_gain.reshape(1, -1), mix_gain.reshape(1, -1), out_w, up_w, down_w)


def solution(mesh):
    placed = (
        P(("sp", "tp"), None),
        P("sp", "tp"),
        P("sp", "tp"),
        P("sp", "tp"),
        P("sp", "tp"),
        P("sp", "tp"),
        P(),
        P("tp", None),
        P(),
        P("sp", "tp"),
        P("sp", "tp"),
    )

    def body(*args):
        return local(mesh.shape["sp"], mesh.shape["tp"], *args)

    if mesh.shape["tp"] == 4 and mesh.shape["sp"] % 2 == 0:
        def whole(*args):
            return fused(mesh.shape["sp"], mesh.shape["tp"], *args)

        return jax.shard_map(whole, mesh=mesh, in_specs=placed, out_specs=P(("sp", "tp"), None), check_vma=False)
    return jax.shard_map(body, mesh=mesh, in_specs=placed, out_specs=P(("sp", "tp"), None), check_vma=False)
```

```python
import functools

import jax
import jax.numpy as jnp
from jax import lax
from jax.experimental import pallas as pl
from jax.experimental.pallas import tpu as pltpu
from jax.sharding import PartitionSpec as P


KEY_CHANNELS = 128
DV = 256
BLOCK = 64
EPS = 1e-06


NT = (((1,), (1,)), ((), ()))
TN = (((0,), (0,)), ((), ()))


def local_states(q_ref, k_ref, v_ref, ld_ref, out_ref, qd_ref, state_ref):
    count = q_ref.shape[0] // BLOCK
    row = lax.broadcasted_iota(jnp.int32, (BLOCK, BLOCK), 0)
    col = lax.broadcasted_iota(jnp.int32, (BLOCK, BLOCK), 1)
    later = (col > row).astype(jnp.float32)
    scale = KEY_CHANNELS ** (-0.5)
    state = jnp.zeros((DV, KEY_CHANNELS), jnp.float32)
    total = jnp.zeros((1, KEY_CHANNELS), jnp.float32)
    for c in range(count):
        rows = pl.ds(c * BLOCK, BLOCK)
        rates = ld_ref[rows, :]
        rest = jnp.dot(later, rates, precision=lax.Precision.HIGHEST, preferred_element_type=jnp.float32)
        last = jnp.sum(rates, axis=0, keepdims=True)
        keys = (k_ref[rows, :].astype(jnp.float32) * jnp.exp(rest)).astype(jnp.bfloat16)
        update = lax.dot_general(v_ref[rows, :], keys, TN, preferred_element_type=jnp.float32)
        state = state * jnp.exp(last) + update
        total = total + last
        q = q_ref[rows, :]
        out_ref[rows, :] = lax.dot_general(
            q, state.astype(jnp.bfloat16), NT, preferred_element_type=jnp.float32
        ) * scale
        qd_ref[rows, :] = (q.astype(jnp.float32) * (jnp.exp(total) * scale)).astype(jnp.bfloat16)
    state_ref[0, :DV, :] = state.astype(jnp.bfloat16)
    state_ref[0, DV:, :] = jnp.broadcast_to(jnp.exp(total), (16, KEY_CHANNELS)).astype(jnp.bfloat16)


def finish_heads(own_ref, qd_ref, state_ref, gate_ref, gain_ref, out_ref):
    readout = own_ref[...] + lax.dot_general(
        qd_ref[...], state_ref[0, :DV, :], NT, preferred_element_type=jnp.float32
    )
    scaled = readout * lax.rsqrt(jnp.mean(readout * readout, axis=-1, keepdims=True) + EPS)
    gates = gate_ref[...].astype(jnp.float32)
    out_ref[...] = (scaled * gain_ref[...] * (gates / (1.0 + jnp.exp(-gates)))).astype(jnp.bfloat16)


def attention_local(q, k, v, ld):
    rows = q.shape[0]
    heads = q.shape[1] // KEY_CHANNELS
    kb = pl.BlockSpec((rows, KEY_CHANNELS), lambda h: (0, h))
    vb = pl.BlockSpec((rows, DV), lambda h: (0, h))
    return pl.pallas_call(
        local_states,
        grid=(heads,),
        in_specs=[kb, kb, vb, kb],
        out_specs=[vb, kb, pl.BlockSpec((1, DV + 16, KEY_CHANNELS), lambda h: (h, 0, 0))],
        out_shape=[
            jax.ShapeDtypeStruct((rows, heads * DV), jnp.float32),
            jax.ShapeDtypeStruct((rows, heads * KEY_CHANNELS), jnp.bfloat16),
            jax.ShapeDtypeStruct((heads, DV + 16, KEY_CHANNELS), jnp.bfloat16),
        ],
        cost_estimate=pl.CostEstimate(flops=6_000_000_000, bytes_accessed=8_000_000, transcendentals=0),
        name="local_states",
    )(q, k, v, ld)


def attention_finish(own, qd, state, gates, gain):
    rows = own.shape[0]
    heads = own.shape[1] // DV
    tile = rows // 2
    vb = pl.BlockSpec((tile, DV), lambda h, r: (r, h))
    return pl.pallas_call(
        finish_heads,
        grid=(heads, rows // tile),
        in_specs=[
            vb,
            pl.BlockSpec((tile, KEY_CHANNELS), lambda h, r: (r, h)),
            pl.BlockSpec((1, DV + 16, KEY_CHANNELS), lambda h, r: (h, 0, 0)),
            vb,
            pl.BlockSpec((1, DV), lambda h, r: (0, 0)),
        ],
        out_specs=vb,
        out_shape=jax.ShapeDtypeStruct(own.shape, jnp.bfloat16),
        cost_estimate=pl.CostEstimate(flops=3_000_000_000, bytes_accessed=4_000_000, transcendentals=0),
        name="finish_heads",
    )(own, qd, state, gates, gain)


def join(earlier, later):
    e, f = earlier.astype(jnp.float32), later.astype(jnp.float32)
    decay = f[:, DV : DV + 1]
    return jnp.concatenate(
        [decay * e[:, :DV] + f[:, :DV], jnp.broadcast_to(decay * e[:, DV : DV + 1], e[:, DV:].shape)], axis=1
    ).astype(jnp.bfloat16)


def shifted(a, by, n):
    return lax.ppermute(a, "sp", [(i, i + by) for i in range(n - by)])


def cycle_of(n):
    return list(range(0, n, 2)) + list(range(n - 1 - n % 2, 0, -2))


class Ring:
    def __init__(self, piece, n):
        self.n, self.cyc, self.piece = n, cycle_of(n), piece
        self.fwd = [(self.cyc[i], self.cyc[(i + 1) % n]) for i in range(n)]
        self.bwd = [(b, a) for a, b in self.fwd]
        self.left = self.right = piece
        self.hops = n // 2

    def hop(self, h):
        left, right = self.left, self.right
        if h == self.hops:
            half = self.piece.shape[0] // 2
            left, right = left[:half], right[half:]
        self.left = lax.ppermute(left, "sp", self.fwd)
        self.right = lax.ppermute(right, "sp", self.bwd)
        if h == self.hops:
            return [jnp.concatenate([self.left, self.right], axis=0)]
        return [self.left, self.right]


def owner_of(n, h):
    cyc = cycle_of(n)
    place = [0] * n
    for i, d in enumerate(cyc):
        place[d] = i
    me = jnp.asarray(place, jnp.int32)[lax.axis_index("sp")]
    cyc = jnp.asarray(cyc, jnp.int32)
    if h == 0:
        return [cyc[me]]
    back = cyc[(me - h) % n]
    return [back] if 2 * h == n else [back, cyc[(me + h) % n]]


def local(
    n_sp, n_tp, stream, query_rows, key_rows, value_rows, gate_rows, log_decay, head_gain, out_weight, mix_gain,
    up_weight, down_weight,
):
    nx = n_tp // 2
    own_rows = stream.shape[0]
    me = lax.axis_index("tp")
    x, core = me // 2, me % 2

    def across(a, dx):
        return lax.ppermute(a, "tp", [(((i // 2 + dx) % nx) * 2 + i % 2, i) for i in range(n_tp)])

    def swap(a):
        return lax.ppermute(a, "tp", [(i ^ 1, i) for i in range(n_tp)])

    up = Ring(up_weight, n_sp)
    down = Ring(down_weight, n_sp)
    width = up_weight.shape[0]
    up_full = lax.dynamic_update_slice_in_dim(
        jnp.zeros((width * n_sp, up_weight.shape[1]), up_weight.dtype), up_weight, owner_of(n_sp, 0)[0] * width, 0
    )
    ups = [up.hop(1)]
    downs = [[down_weight]]

    def tie(a, ring):
        a, ring.left, ring.right = lax.optimization_barrier((a, ring.left, ring.right))
        return a

    w = {(0, 0): out_weight}
    for dx in range(1, nx):
        w[dx, 0] = across(out_weight, dx)
    for dx in range(nx):
        w[dx, 1] = swap(w[dx, 0])

    own, qd, summary = attention_local(query_rows, key_rows, value_rows, log_decay)
    before, covered = tie(shifted(summary, 1, n_sp), up), 1
    while covered < n_sp - 1:
        wider = join(before, summary)
        if len(ups) < up.hops - 1:
            ups.append(up.hop(len(ups) + 1))
        before, covered = join(shifted(wider, covered + 1, n_sp), before), 2 * covered + 1
        before = tie(before, up)
    while len(ups) < up.hops:
        ups.append(up.hop(len(ups) + 1))
    before, down.left, down.right = lax.optimization_barrier((before, down.left, down.right))
    downs.append(down.hop(1))
    heads_out = attention_finish(own, qd, before, gate_rows, head_gain.reshape(1, DV))

    attn = None
    for dx in range(nx):
        for dc in range(2):
            to = ((x - dx) % nx) * 2 + (core + dc) % 2
            block = lax.dynamic_slice_in_dim(heads_out, to * own_rows, own_rows, 0)
            if (dx, dc) != (0, 0):
                block = lax.ppermute(
                    block, "tp", [(((i // 2 + dx) % nx) * 2 + (i % 2 + dc) % 2, i) for i in range(n_tp)]
                )
            term = jnp.dot(block, w[dx, dc], preferred_element_type=jnp.float32)
            attn = term if attn is None else attn + term
    midf = (stream.astype(jnp.float32) + attn).astype(jnp.bfloat16).astype(jnp.float32)
    normed = (
        midf * lax.rsqrt(jnp.mean(midf * midf, axis=-1, keepdims=True) + EPS) * mix_gain
    ).astype(jnp.bfloat16)

    normed = tie(normed, down)
    downs.append(down.hop(2))

    for h, pieces in enumerate(ups, 1):
        for piece, who in zip(pieces, owner_of(n_sp, h)):
            up_full = lax.dynamic_update_slice_in_dim(up_full, piece, who * width, 0)

    n = {(0, 0): normed}
    for dx in range(1, nx):
        n[dx, 0] = across(normed, dx)
    for dx in range(nx):
        n[dx, 1] = swap(n[dx, 0])
    n[nx - 1, 1] = tie(n[nx - 1, 1], down)
    while len(downs) <= down.hops:
        downs.append(down.hop(len(downs)))
    order = [(dx, dc) for dc in range(2) for dx in range(nx)]

    def hidden_of(rows):
        pre = jnp.dot(rows, up_full, preferred_element_type=jnp.float32)
        return jnp.square(jax.nn.relu(pre)).astype(jnp.bfloat16)

    hiddens = []
    for key in order:
        hiddens.append(hidden_of(n[key]))
    hidden = jnp.concatenate(hiddens, axis=0)

    out = jnp.zeros(stream.shape, jnp.bfloat16)
    mid = midf.astype(jnp.bfloat16)
    for h, pieces in enumerate(downs):
        whole = jnp.concatenate(pieces, axis=0) if len(pieces) > 1 else pieces[0]
        part = lax.dot_general(hidden, whole, NT, preferred_element_type=jnp.float32).astype(jnp.bfloat16)
        hidden, part = lax.optimization_barrier((hidden, part))
        half = nx * own_rows
        both = part[:half].astype(jnp.float32) + swap(part[half:]).astype(jnp.float32)
        feed = both[:own_rows]
        for dx in range(1, nx):
            send = both[dx * own_rows : (dx + 1) * own_rows].astype(jnp.bfloat16)
            feed = feed + across(send, nx - dx).astype(jnp.float32)
        for j, who in enumerate(owner_of(n_sp, h)):
            cols = lax.dynamic_slice_in_dim(mid, who * width, width, 1).astype(jnp.float32)
            done = (cols + feed[:, j * width : (j + 1) * width]).astype(jnp.bfloat16)
            out = lax.dynamic_update_slice_in_dim(out, done, who * width, 1)
    return out


UP_TILE = 512
CUT = 2
MESH = pl.DeviceIdType.MESH


class Links:
    def __init__(self, n_sp):
        self.sp, self.tp = lax.axis_index("sp"), lax.axis_index("tp")
        self.nz = n_sp // 2
        self.z, self.y = self.sp // 2, self.sp % 2
        self.x, self.c = self.tp // 2, self.tp % 2
        self.core = (self.sp, self.x * 2 + 1 - self.c)
        self.xn = (self.sp, (1 - self.x) * 2 + self.c)
        self.xo = (self.sp, (1 - self.x) * 2 + 1 - self.c)
        self.yn = (self.z * 2 + 1 - self.y, self.tp)

    def at_z(self, z):
        return (z * 2 + self.y, self.tp)

    def piece(self, s):
        z, n = self.z, self.nz
        near = jnp.minimum(z, n - 1 - z)
        turn = jnp.where(s % 2 == 1, z - (s + 1) // 2, z + s // 2)
        rest = jnp.where(z < n - 1 - z, s, n - 1 - s)
        return jnp.where(s <= 2 * near, turn, rest)


def remote(src, dst, send, recv, dev):
    return pltpu.make_async_remote_copy(
        src_ref=src, dst_ref=dst, send_sem=send, recv_sem=recv, device_id=dev, device_id_type=MESH
    )


def layer_kernel(
    n_sp, n_tp, stream, query, key, value, gate, rates_in, head_gain, mix_gain, out_w, up_w, down_w, out,
    up, down, wo, qv, kv, vv, gv, ldv, own, qd, state, total, summ, peer, tsend, trecv, prefix, bsend, before,
    heads, hrecv, acts, hidden, mid, psend, pown, sum_x, sum_y, pass_y, pass_x,
    gain_h, gain_m, ld_s, zown_s, zfwd_s, z_r, y_s, y_r, d_s, du_r, dd_r, wo_s, wo_r, s_s, s_r, t_s, t_r, h_s, h_r, a_s, a_r,
    p_s, p_r,
):
    f32, bf16 = jnp.float32, jnp.bfloat16
    L = Links(n_sp)
    z, y, c, nz = L.z, L.y, L.c, L.nz
    rows, width = stream.shape
    span = query.shape[0]
    n_heads = query.shape[1] // KEY_CHANNELS
    slab, half = up_w.shape[0], up_w.shape[1] // 2
    half_rows = rows // 2
    fine = slab // CUT

    barrier = pltpu.get_barrier_semaphore()
    partners = [L.core, L.xn, L.xo, L.yn]
    for dev in partners:
        pl.semaphore_signal(barrier, inc=1, device_id=dev, device_id_type=MESH)
    for has, to in ((z > 0, z - 1), (z < nz - 1, z + 1)):
        @pl.when(has)
        def _():
            pl.semaphore_signal(barrier, inc=1, device_id=L.at_z((to + nz) % nz), device_id_type=MESH)

    loads = [(query, qv), (key, kv), (value, vv), (rates_in, ldv)]
    first = [pltpu.make_async_copy(a, b, ld_s.at[i]) for i, (a, b) in enumerate(loads)]
    for cp in first:
        cp.start()
    ends = jnp.where(z > 0, 1, 0) + jnp.where(z < nz - 1, 1, 0)
    pl.semaphore_wait(barrier, len(partners) + ends)

    bufs, source, cuts = (up, down), (up_w, down_w), (1, CUT)

    def place(kind, core, j, part, n=1):
        size = slab // cuts[kind]
        return bufs[kind].at[
            pl.ds(pl.multiple_of((j * 2 * cuts[kind] + part) * size, size), n * size),
            pl.ds(pl.multiple_of(core * half, half), half),
        ]

    def halfcols(kind, h, cut=None):
        size = slab // cuts[kind]
        return source[kind].at[pl.ds(0, slab) if cut is None else pl.ds(cut * size, size), pl.ds(pl.multiple_of(h * half, half), half)]

    def whole_part(kind, yy):
        return place(kind, c, z, yy * cuts[kind], cuts[kind])

    keep = [pltpu.make_async_copy(halfcols(k, y), whole_part(k, y), ld_s.at[6 + k]) for k in range(2)]
    cross = [remote(halfcols(k, 1 - y), whole_part(k, y), y_s.at[0], y_r.at[k], L.yn) for k in range(2)]

    def z_slot(kind, part):
        return part + 2 * kind

    def to_side(kind, far, cut, side):
        part = (1 - y if far else y) * cuts[kind] + cut
        src = place(kind, c, z, part) if far else halfcols(kind, y, cut)
        to = L.at_z((z + (1 if side else -1) + nz) % nz)
        return remote(src, place(kind, c, z, part), zown_s.at[side], z_r.at[z, z_slot(kind, part)], to)

    final = (2 * nz - 1) * CUT

    def core_r(kind, s, part):
        if kind == 0:
            return du_r.at[0]
        u = s * 2 * CUT + part
        return dd_r.at[jnp.where(u < final, u // CUT, final // CUT + u - final)]

    def to_core(kind, s, part, cut=None):
        dst = place(kind, c, L.piece(s), part)
        src = dst if cut is None else halfcols(kind, y, cut)
        return remote(src, dst, d_s.at[kind], core_r(kind, s, part), L.core)

    def send_own(kind, far, sides=(0, 1)):
        for side in sides:
            @pl.when((z < nz - 1) if side else (z > 0))
            def _():
                for cut in range(cuts[kind]):
                    to_side(kind, far, cut, side).start()

    def share_own(kind, far):
        for cut in range(cuts[kind]):
            to_core(kind, 0, (1 - y if far else y) * cuts[kind] + cut, None if far else cut).start()

    def onward(kind, j, part):
        to = jnp.where(j < z, z + 1, z - 1)
        dst = place(kind, c, j, part)
        return remote(dst, dst, zfwd_s.at[kind], z_r.at[j, z_slot(kind, part)], L.at_z((to + nz) % nz))

    inner = jnp.logical_and(z > 0, z < nz - 1)
    edge = jnp.logical_or(z == 0, z == nz - 1)

    def arrive(kind, s, part, forward):
        j = L.piece(s)
        cp = onward(kind, j, part)
        cp.wait_recv()
        if forward:
            cp.start()
        to_core(kind, s, part).start()

    def forward_inner(kind, s, part):
        @pl.when(inner)
        def _():
            arrive(kind, s, part, True)

    def arrive_edge(kind, s, part):
        @pl.when(edge)
        def _():
            arrive(kind, s, part, False)

    send_own(0, 0)
    send_own(1, 0, (0,))
    wo_half, wo_quarter = out_w.shape[0] // 2, out_w.shape[0] // 4

    def wo_rows(k):
        return pl.ds(0, wo_half) if k is None else pl.ds(pl.multiple_of(wo_half + k * wo_quarter, wo_quarter), wo_quarter)

    wo_own = pltpu.make_async_copy(out_w, wo.at[L.tp], ld_s.at[4])
    wo_c = remote(out_w, wo.at[L.tp], wo_s.at[0], wo_r.at[1], L.core)
    wo_b = remote(out_w.at[wo_rows(y), :], wo.at[L.tp, wo_rows(y), :], wo_s.at[0], wo_r.at[3], L.xn)
    wo_a = remote(out_w.at[wo_rows(None), :], wo.at[L.tp, wo_rows(None), :], wo_s.at[0], wo_r.at[0], L.xn)

    def wo_pass(k):
        ref = wo.at[L.xn[1], wo_rows(k), :]
        return remote(ref, ref, wo_s.at[0], wo_r.at[4], L.yn)

    wo_b.start()
    wo_a.start()
    wo_c.start()
    wo_own.start()
    for k in range(2):
        keep[k].start()
        share_own(k, 0)
    late = [pltpu.make_async_copy(gate, gv, ld_s.at[5]), pltpu.make_async_copy(stream, mid, ld_s.at[8])]
    late += [pltpu.make_async_copy(head_gain, gain_h, ld_s.at[9]), pltpu.make_async_copy(mix_gain, gain_m, ld_s.at[10])]
    for cp in late:
        cp.start()

    row = lax.broadcasted_iota(jnp.int32, (BLOCK, BLOCK), 0)
    col = lax.broadcasted_iota(jnp.int32, (BLOCK, BLOCK), 1)
    later = (col > row).astype(f32)
    scale = KEY_CHANNELS ** (-0.5)
    state[...] = jnp.zeros_like(state)
    total[...] = jnp.zeros_like(total)
    for cp in first:
        cp.wait()

    def block(i, carry):
        at = pl.ds(pl.multiple_of(i * BLOCK, BLOCK), BLOCK)
        for h in range(n_heads):
            ks, vs = pl.ds(h * KEY_CHANNELS, KEY_CHANNELS), pl.ds(h * DV, DV)
            rates = ldv[at, ks]
            rest = jnp.dot(later, rates, precision=lax.Precision.HIGHEST, preferred_element_type=f32)
            last = jnp.sum(rates, axis=0, keepdims=True)
            keys = (kv[at, ks].astype(f32) * jnp.exp(rest)).astype(bf16)
            update = lax.dot_general(vv[at, vs], keys, TN, preferred_element_type=f32)
            new = state[h] * jnp.exp(last) + update
            state[h] = new
            tot = total[h] + last
            total[h] = tot
            q = qv[at, ks]
            own[at, vs] = lax.dot_general(q, new.astype(bf16), NT, preferred_element_type=f32) * scale
            qd[at, ks] = (q.astype(f32) * (jnp.exp(tot) * scale)).astype(bf16)
        return carry

    lax.fori_loop(0, span // BLOCK, block, 0, unroll=4)
    for h in range(n_heads):
        summ[h, :DV, :] = state[h].astype(bf16)
        summ[h, DV:, :] = jnp.broadcast_to(jnp.exp(total[h]), (16, KEY_CHANNELS)).astype(bf16)

    swap = remote(summ.at[1 - y], peer, s_s.at[0], s_r.at[0], L.yn)
    swap.start()
    cross[0].start()
    swap.wait_recv()
    mine, other = summ[y].astype(f32), peer[...].astype(f32)
    is0 = y == 0
    early, late_ = jnp.where(is0, mine, other), jnp.where(is0, other, mine)
    dec = late_[DV : DV + 1]
    here = dec * early[:DV] + late_[:DV]
    onto_here = dec * early[DV : DV + 1]

    def hand_on(to):
        return remote(tsend, trecv, t_s.at[0], t_r.at[0], L.at_z((to + nz) % nz))

    @pl.when(z == nz - 2)
    def _():
        to_side(1, 0, 0, 1).start()

    prefix[...] = jnp.zeros_like(prefix)

    @pl.when(z > 0)
    def _():
        hand_on(z).wait_recv()
        prefix[...] = trecv[...].astype(f32)

    whole = prefix[...]

    @pl.when(z < nz - 1)
    def _():
        tsend[...] = (onto_here * whole + here).astype(bf16)
        hand_on(z + 1).start()
        for cut in range(1, CUT):
            to_side(1, 0, cut, 1).start()

    @pl.when(z < nz - 2)
    def _():
        to_side(1, 0, 0, 1).start()

    first_y = jnp.where(is0, mine, other)
    onto = first_y[DV : DV + 1] * whole + first_y[:DV]
    bsend[...] = jnp.where(is0, onto, whole).astype(bf16)
    before[y] = jnp.where(is0, whole, onto).astype(bf16)
    back = remote(bsend, before.at[y], s_s.at[1], s_r.at[1], L.yn)
    back.start()
    wo_from_b = remote(out_w.at[wo_rows(y), :], wo.at[L.xn[1], wo_rows(y), :], wo_s.at[0], wo_r.at[3], L.xn)
    wo_from_b.wait_recv()
    wo_pass(y).start()
    cross[1].start()
    cross[0].wait_recv()
    send_own(0, 1)
    share_own(0, 1)
    forward_inner(0, 1, y)
    forward_inner(0, 2, y)
    remote(bsend, before.at[1 - y], s_s.at[1], s_r.at[1], L.yn).wait_recv()
    late[0].wait()
    late[2].wait()
    gain = gain_h[...]

    def finish(t):
        for r in range(0, rows, 128):
            at = pl.ds(pl.multiple_of(t * rows + r, 128), 128)
            for h in range(n_heads):
                ks, vs = pl.ds(h * KEY_CHANNELS, KEY_CHANNELS), pl.ds(h * DV, DV)
                readout = own[at, vs] + lax.dot_general(qd[at, ks], before[h], NT, preferred_element_type=f32)
                scaled = readout * lax.rsqrt(jnp.mean(readout * readout, axis=-1, keepdims=True) + EPS)
                g = gv[at, vs].astype(f32)
                heads[t, pl.ds(r, 128), vs] = (scaled * gain * (g / (1.0 + jnp.exp(-g)))).astype(bf16)

    for dev in (L.xn, L.xo, L.core):
        t = dev[1]
        finish(t)
        cp = remote(heads.at[t], hrecv.at[L.tp], h_s.at[0], h_r.at[0], dev)
        cp.start()
    finish(L.tp)
    hrecv[L.tp] = heads[L.tp]
    forward_inner(0, 1, 1 - y)
    forward_inner(0, 2, 1 - y)

    remote(out_w.at[wo_rows(None), :], wo.at[L.xn[1], wo_rows(None), :], wo_s.at[0], wo_r.at[0], L.xn).wait_recv()
    wo_pass(1 - y).wait_recv()
    relay = remote(wo.at[L.xn[1]], wo.at[L.xn[1]], wo_s.at[0], wo_r.at[2], L.core)
    relay.start()
    remote(out_w, wo.at[L.core[1]], wo_s.at[0], wo_r.at[1], L.core).wait_recv()
    remote(wo.at[L.xo[1]], wo.at[L.xo[1]], wo_s.at[0], wo_r.at[2], L.core).wait_recv()
    wo_own.wait()
    late[1].wait()
    late[3].wait()
    forward_inner(0, 3, y)
    arrive_edge(0, 1, y)
    arrive_edge(0, 1, 1 - y)
    others = pl.ds(0, n_tp - 1)
    all_heads = remote(heads.at[others], hrecv.at[others], h_s.at[0], h_r.at[0], L.xn)
    all_heads.wait_recv()

    square = jnp.zeros((rows, 1), f32)
    wide = min(512, width)
    for n in range(0, width, wide):
        cols = pl.ds(n, wide)
        acc = mid[:, cols].astype(f32)
        for t in range(n_tp):
            acc = acc + jnp.dot(hrecv[t], wo[t, :, cols], preferred_element_type=f32)
        m = acc.astype(bf16)
        mid[:, cols] = m
        m = m.astype(f32)
        square = square + jnp.sum(m * m, axis=-1, keepdims=True)
    norm = lax.rsqrt(square * (1.0 / width) + EPS)
    for n in range(0, width, wide):
        cols = pl.ds(n, wide)
        acts[:rows, cols] = (mid[:, cols].astype(f32) * norm * gain_m[:, cols]).astype(bf16)

    a, b = pl.ds(0, half_rows), pl.ds(half_rows, half_rows)

    def act_copy(i):
        slot, part, dst, dev = [(0, 0, 1, L.xn), (0, 1, 1, L.xn), (0, 0, 2, L.yn), (0, 1, 2, L.yn), (1, 0, 3, L.yn), (2, 1, 3, L.xn)][i]
        src = acts.at[pl.ds(slot * rows + part * half_rows, half_rows), :]
        return remote(src, acts.at[pl.ds(dst * rows + part * half_rows, half_rows), :], a_s.at[0], a_r.at[(0, 2, 2, 1, 2, 2)[i]], dev)

    for i in (0, 3, 1, 2):
        act_copy(i).start()
    forward_inner(0, 3, 1 - y)
    cross[1].wait_recv()
    send_own(1, 1)
    share_own(1, 1)
    act_copy(0).wait_recv()
    act_copy(4).start()
    act_copy(3).wait_recv()
    act_copy(5).start()
    for s in (1, 2):
        for part in range(2 * CUT):
            forward_inner(1, s, part)
    arrive_edge(0, 2, y)
    arrive_edge(0, 2, 1 - y)
    rest = acts.at[pl.ds(0, 2 * rows), :]
    remote(rest, rest, a_s.at[0], a_r.at[2], L.xn).wait_recv()
    for part in range(CUT):
        forward_inner(1, 3, part)

    arrive_edge(0, 3, y)
    arrive_edge(0, 3, 1 - y)
    keep[0].wait()
    theirs = up.at[:, pl.ds(pl.multiple_of((1 - c) * half, half), half)]
    remote(theirs, theirs, d_s.at[0], du_r.at[0], L.core).wait_recv()

    def up_step(n, carry):
        at = pl.ds(pl.multiple_of(n * UP_TILE, UP_TILE), UP_TILE)
        pre = jnp.maximum(jnp.dot(acts[...], up[:, at], preferred_element_type=f32), 0.0)
        hidden[:, at] = (pre * pre).astype(bf16)
        return carry

    lax.fori_loop(0, 2 * half // UP_TILE, up_step, 0)
    for part in range(CUT, 2 * CUT):
        forward_inner(1, 3, part)
    keep[1].wait()

    steps = 2 * nz * CUT

    def columns(u, n=1):
        d = (L.piece(u // (2 * CUT)) * 2 * CUT + u % (2 * CUT)) * fine
        return pl.ds(pl.multiple_of(d, fine), n * fine)

    def part_copy(i, u):
        cols = columns(u)
        src, dst, dev = [
            (psend.at[2, a, cols], pass_y.at[:, cols], L.yn),
            (psend.at[2, b, cols], pass_x.at[:, cols], L.xn),
            (psend.at[0, b, cols], sum_x.at[b, cols], L.xn),
            (psend.at[1, a, cols], sum_y.at[a, cols], L.yn),
            (psend.at[0, a, cols], sum_x.at[a, cols], L.xn),
            (psend.at[1, b, cols], sum_y.at[b, cols], L.yn),
        ][i]
        return remote(src, dst, p_s.at[0], p_r.at[0 if i < 2 else 1, u], dev)

    def terms_of(u, n):
        s = u // (2 * CUT)

        @pl.when(jnp.logical_and(edge, s > 0))
        def _():
            for k in range(n):
                arrive(1, s, u % (2 * CUT) + k, False)

        cols = columns(u, n)
        got_here, got_there = (pl.ds(pl.multiple_of(k * half, half), half) for k in (c, 1 - c))

        def product(units):
            return lax.dot_general(hidden[:, units], down[cols, units], NT, preferred_element_type=f32)

        terms = product(got_here) if n == 1 else None
        theirs = down.at[cols, got_there]
        remote(theirs, theirs, d_s.at[1], core_r(1, s, u % (2 * CUT)), L.core).wait_recv()
        terms = product(pl.ds(0, 2 * half)) if terms is None else terms + product(got_there)
        pown[:, cols] = terms[:rows]
        for i in range(3):
            psend[i, :, cols] = terms[(i + 1) * rows : (i + 2) * rows].astype(bf16)
        for i in range(4):
            for k in range(n):
                part_copy(i, u + k).start()

    def pass_on(u):
        cols = columns(u)
        passed = psend.at[0, :, cols]
        remote(passed, passed, p_s.at[0], p_r.at[0, u], L.xn).wait_recv()
        psend[0, a, cols] = (psend[0, a, cols].astype(f32) + pass_y[:, cols].astype(f32)).astype(bf16)
        part_copy(4, u).start()
        psend[1, b, cols] = (psend[1, b, cols].astype(f32) + pass_x[:, cols].astype(f32)).astype(bf16)
        part_copy(5, u).start()

    def close(u):
        cols = columns(u)
        sums = psend.at[pl.ds(0, 2), :, cols]
        remote(sums, sums, p_s.at[0], p_r.at[1, u], L.xn).wait_recv()
        feed = pown[:, cols] + sum_x[:, cols].astype(f32) + sum_y[:, cols].astype(f32)
        out[:, cols] = (mid[:, cols].astype(f32) + feed).astype(bf16)

    def passed_after(u):
        return jnp.where(u < final - 1, jnp.maximum(u - CUT + 1, 0), jnp.where(u < steps - 1, final, steps))

    def closed_after(u):
        return jnp.where(u < final, jnp.maximum(u - 2 * CUT + 1, 0), jnp.where(u < steps - 1, final, steps))

    def down_step(u, carry):
        @pl.when(jnp.logical_and(u < final, u % CUT == 0))
        def _():
            terms_of(u, CUT)

        @pl.when(u >= final)
        def _():
            terms_of(u, 1)

        lax.fori_loop(passed_after(u - 1), passed_after(u), lambda v, _: pass_on(v), None)
        lax.fori_loop(closed_after(u - 1), closed_after(u), lambda v, _: close(v), None)
        return carry

    lax.fori_loop(0, steps, down_step, 0)

    def sent(ref, sem):
        remote(ref, ref, sem, sem, L.core).wait_send()

    mine_cols = pl.ds(0, half)
    sent(up.at[pl.ds(0, 2 * slab), mine_cols], y_s.at[0])
    for side in range(2):
        @pl.when((z < nz - 1) if side else (z > 0))
        def _():
            sent(up.at[pl.ds(0, 4 * slab), mine_cols], zown_s.at[side])
    for k in range(2):
        sent(up.at[:, mine_cols], d_s.at[k])

        @pl.when(inner)
        def _():
            sent(up.at[pl.ds(0, 2 * slab * (nz - 1)), mine_cols], zfwd_s.at[k])
    sent(wo.at[pl.ds(0, 3)], wo_s.at[0])
    swap.wait_send()
    back.wait_send()

    @pl.when(z < nz - 1)
    def _():
        hand_on(z + 1).wait_send()

    all_heads.wait_send()
    sent(acts.at[pl.ds(0, 3 * rows), :], a_s.at[0])
    sent(psend, p_s.at[0])


def fused(
    n_sp, n_tp, stream, query, key, value, gate, rates, head_gain, out_w, mix_gain, up_w, down_w
):
    f32, bf16 = jnp.float32, jnp.bfloat16
    rows, width = stream.shape
    n_heads = query.shape[1] // KEY_CHANNELS
    half = up_w.shape[1] // 2
    nz, np_ = n_sp // 2, n_sp * CUT
    K = KEY_CHANNELS
    V, D = pltpu.VMEM, pltpu.SemaphoreType.DMA
    hbm = pl.BlockSpec(memory_space=pltpu.HBM)
    vmem = pl.BlockSpec(memory_space=pltpu.VMEM)
    return pl.pallas_call(
        functools.partial(layer_kernel, n_sp, n_tp),
        out_shape=pltpu.VMEM((rows, width), bf16),
        in_specs=[hbm] * 11,
        out_specs=vmem,
        scratch_shapes=[
            V((width, 2 * half), bf16), V((width, 2 * half), bf16), V((n_tp, out_w.shape[0], width), bf16),
            V(query.shape, bf16), V(key.shape, bf16), V(value.shape, bf16), V(gate.shape, bf16), V(rates.shape, f32),
            V(value.shape, f32), V(query.shape, bf16), V((n_heads, DV, K), f32), V((n_heads, 1, K), f32),
            V((n_heads, DV + 16, K), bf16), V((DV + 16, K), bf16), V((DV, K), bf16), V((DV, K), bf16),
            V((DV, K), f32), V((DV, K), bf16), V((n_heads, DV, K), bf16),
            V((n_tp, rows, value.shape[1]), bf16), V((n_tp, rows, value.shape[1]), bf16),
            V((4 * rows, width), bf16), V((4 * rows, 2 * half), bf16), V((rows, width), bf16),
            V((3, rows, width), bf16), V((rows, width), f32), V((rows, width), bf16), V((rows, width), bf16),
            V((rows // 2, width), bf16), V((rows // 2, width), bf16),
            V((1, head_gain.shape[0]), f32), V((1, width), f32),
            D((11,)), D((2,)), D((2,)), D((nz, 2 + 2 * CUT)), D((1,)), D((2,)), D((2,)), D((1,)), D((2 * nz - 1 + CUT,)),
            D((1,)), D((5,)), D((2,)), D((2,)), D((1,)), D((1,)), D((1,)), D((1,)), D((1,)), D((3,)), D((1,)), D((2, np_)),
        ],
        compiler_params=pltpu.CompilerParams(
            collective_id=0, has_side_effects=True, vmem_limit_bytes=58_000_000
        ),
        name="layer",
    )(stream, query, key, value, gate, rates, head_gain.reshape(1, -1), mix_gain.reshape(1, -1), out_w, up_w, down_w)


def solution(mesh):
    placed = (
        P(("sp", "tp"), None),
        P("sp", "tp"),
        P("sp", "tp"),
        P("sp", "tp"),
        P("sp", "tp"),
        P("sp", "tp"),
        P(),
        P("tp", None),
        P(),
        P("sp", "tp"),
        P("sp", "tp"),
    )

    def body(*args):
        return local(mesh.shape["sp"], mesh.shape["tp"], *args)

    if mesh.shape["tp"] == 4 and mesh.shape["sp"] % 2 == 0:
        def whole(*args):
            return fused(mesh.shape["sp"], mesh.shape["tp"], *args)

        return jax.shard_map(whole, mesh=mesh, in_specs=placed, out_specs=P(("sp", "tp"), None), check_vma=False)
    return jax.shard_map(body, mesh=mesh, in_specs=placed, out_specs=P(("sp", "tp"), None), check_vma=False)
```
